32 devices in a mesh: ep: 32 (over z, y, x, core).
Axes of the slice: x: 2, y: 2, z: 4, core: 2. Of those that a mesh axis runs over, the one named last changes fastest.
Arguments:
- tokens: bfloat16 [1536, 2048], P('ep'), may hold values from -6 to 6
- history_length: int32 [1536], P('ep'), may hold values from 1024 to 8192
- norm_gain: float32 [2048], replicated, may hold values from 0.1 to 1.9
- w_query: bfloat16 [2048, 512], replicated, may hold values from -0.125 to 0.125
- w_key: bfloat16 [2048, 512], replicated, may hold values from -0.125 to 0.125
- w_value: bfloat16 [2048, 512], replicated, may hold values from -0.125 to 0.125
- w_gate: bfloat16 [2048, 512], replicated, may hold values from -0.125 to 0.125
- decay_rate: float32 [8], replicated, may hold values from 0.003 to 0.7
- state: float32 [1536, 8, 64, 64], P('ep'), may hold values from -4 to 4
- head_gain: float32 [512], replicated, may hold values from 0.1 to 1.9
- w_out: bfloat16 [512, 2048], replicated, may hold values from -0.25 to 0.25
- moe_gain: float32 [2048], replicated, may hold values from 0.1 to 1.9
- route_weights: float32 [1536, 2], P('ep'), may hold values from 0.3 to 3
- expert_group: int32 [1536], P('ep'), may hold values from 0 to 3, as said below
- expert_inner: int32 [1536, 2], P('ep'), may hold values from 0 to 7, as said below
- expert_gate: bfloat16 [32, 2048, 256], P('ep'), may hold values from -0.125 to 0.125
- expert_up: bfloat16 [32, 2048, 256], P('ep'), may hold values from -0.125 to 0.125
- expert_down: bfloat16 [32, 256, 2048], P('ep'), may hold values from -0.375 to 0.375
Outputs:
- output: bfloat16 [1536, 2048], P('ep')
- new_state: float32 [1536, 8, 64, 64], P('ep')
The draws below stay inside these ranges and needn't reach their ends.
Inputs may be any that keep to these rules, and one draw needn't show every extreme that they name: `expert_group`: together with expert_inner it names 2 different experts of one group for each token. `expert_inner`: the rows of one device name one expert at most 6 times; in every draw some expert is named exactly 6 times by the rows of every device.
All inputs are finite; a program needn't handle non-finite values.
Results may differ from the reference program's by a relative error of at most 0.02.
Values may be sent and summed in bfloat16 or wider, within the bound.
A program may use at most 128 MiB of HBM per device.

```python
import math
import jax
import jax.numpy as jnp
from jax import lax

D = 2048
HEADS = 8
HEAD_DIM = 64
RET_WIDTH = 512
EXPERT_WIDTH = 256
SEQ_DEV = 48
TOKENS = 1536
EXPERTS = 32
GROUPS = 4
GROUP_SIZE = 8
TOP_K = 2
CAP = 6
N_EP = 32


def route_table(key):
    root_key = jax.random.fold_in(key, 7)
    pair_count = EXPERTS * CAP // 2
    per_group = pair_count // GROUPS
    hot_group = jax.random.randint(jax.random.fold_in(root_key, 1), (), 0, GROUPS)
    relabel = jax.vmap(lambda subkey: jax.random.permutation(subkey, GROUP_SIZE))(jax.random.split(jax.random.fold_in(root_key, 2), GROUPS))
    pair_ids = jnp.arange(pair_count, dtype=jnp.int32)
    pair_group = pair_ids // per_group
    pair_offset = pair_ids % per_group
    first_inner = relabel[pair_group, 2 * pair_offset % GROUP_SIZE]
    second_inner = relabel[pair_group, (2 * pair_offset + 1) % GROUP_SIZE]
    heated = (pair_group == hot_group) & (pair_offset % (GROUP_SIZE // 2) == 0)

    def one_block(subkey):
        jitter = jax.random.randint(jax.random.fold_in(subkey, 1), (pair_count,), 0, 1 << 20)
        scores = jnp.where(heated, pair_ids, (jitter + 1) * pair_count + pair_ids)
        _, chosen = lax.top_k(-scores, SEQ_DEV)
        chosen = chosen[jax.random.permutation(jax.random.fold_in(subkey, 2), SEQ_DEV)]
        return (pair_group[chosen], jnp.stack([first_inner[chosen], second_inner[chosen]], axis=-1))
    groups, inner_ids = jax.vmap(one_block)(jax.random.split(jax.random.fold_in(root_key, 3), TOKENS // SEQ_DEV))
    return (groups.reshape(TOKENS).astype(jnp.int32), inner_ids.reshape(TOKENS, TOP_K).astype(jnp.int32))


def draw_expert_group(key, part):
    return route_table(key)[0]


def draw_expert_inner(key, part):
    return route_table(key)[1]


def place_ends(result, own_key, least, largest):
    dims = result.shape
    index_at = [jax.random.randint(jax.random.fold_in(own_key, axis), (), 0, dims[axis]) for axis in range(len(dims))]
    result = result.at[tuple(index_at)].set(least)
    longest = dims.index(max(dims))
    index_at[longest] = (index_at[longest] + 1) % dims[longest]
    return result.at[tuple(index_at)].set(largest)


def block_levels(own_key, extent, cuts, low, high):
    level = 1.0
    for position, shards_of in cuts:
        steps = jax.random.uniform(jax.random.fold_in(jax.random.fold_in(own_key, 6), position), (shards_of,), jnp.float32, low / len(cuts), high / len(cuts))
        level = level * jnp.repeat(jnp.exp(steps), extent[position] // shards_of).reshape((-1,) + (1,) * (len(extent) - 1 - position))
    return level


def normal_values(own_key, extent, scale, most, cuts=(), held_as=jnp.bfloat16):
    values = scale * jax.random.normal(own_key, extent, jnp.float32)
    if cuts:
        values = values * block_levels(own_key, extent, cuts, -0.22, 0.18)
    return jnp.clip(values, -most, most).astype(held_as)


def setup_inputs(seed: int = 0) -> dict:
    key_list = jax.random.split(jax.random.key(seed), 19)
    return {
        "tokens": normal_values(key_list[0], (TOKENS, D), 1.0, 6.0, ((0, 32),)),
        "history_length": place_ends(jax.random.randint(key_list[1], (TOKENS,), 1024, 8193), jax.random.fold_in(key_list[1], 1), 1024, 8192).astype(jnp.int32),
        "norm_gain": jnp.clip(1.0 + 0.18 * jax.random.normal(key_list[2], (D,), jnp.float32), 0.1, 1.9),
        "w_query": normal_values(key_list[3], (D, RET_WIDTH), D ** -0.5, 0.125),
        "w_key": normal_values(key_list[4], (D, RET_WIDTH), D ** -0.5, 0.125),
        "w_value": normal_values(key_list[5], (D, RET_WIDTH), D ** -0.5, 0.125),
        "w_gate": normal_values(key_list[6], (D, RET_WIDTH), D ** -0.5, 0.125),
        "decay_rate": jnp.clip(jnp.exp(jax.random.uniform(key_list[7], (HEADS,), jnp.float32, math.log(0.003), math.log(0.7))), 0.003, 0.7),
        "state": normal_values(key_list[8], (TOKENS, HEADS, HEAD_DIM, HEAD_DIM), 0.3, 4.0, ((0, 32),), jnp.float32),
        "head_gain": jnp.clip(1.0 + 0.18 * jax.random.normal(key_list[9], (RET_WIDTH,), jnp.float32), 0.1, 1.9),
        "w_out": normal_values(key_list[10], (RET_WIDTH, D), RET_WIDTH ** -0.5, 0.25),
        "moe_gain": jnp.clip(1.0 + 0.18 * jax.random.normal(key_list[11], (D,), jnp.float32), 0.1, 1.9),
        "route_weights": jnp.clip(jnp.exp(math.log(3.0) - 2.3025851 * jax.random.uniform(key_list[12], (TOKENS, TOP_K), jnp.float32) ** block_levels(key_list[12], (TOKENS, TOP_K), ((0, 32),), -0.2, 0.2)), 0.3, 3.0),
        "expert_group": draw_expert_group(jax.random.fold_in(key_list[18], 71), 0),
        "expert_inner": draw_expert_inner(jax.random.fold_in(key_list[18], 71), 0),
        "expert_gate": normal_values(key_list[15], (EXPERTS, D, EXPERT_WIDTH), D ** -0.5, 0.125, ((0, 32),)),
        "expert_up": normal_values(key_list[16], (EXPERTS, D, EXPERT_WIDTH), D ** -0.5, 0.125, ((0, 32),)),
        "expert_down": normal_values(key_list[17], (EXPERTS, EXPERT_WIDTH, D), EXPERT_WIDTH ** -0.5, 0.375, ((0, 32),)),
    }


epsilon = 1e-06

def rotate(values, places):
    halfway = values.shape[-1] // 2
    inverse = 10000.0 ** (-jnp.arange(halfway, dtype=jnp.float32) / halfway)
    angles = places[:, None] * inverse[None, :]
    cosine = jnp.cos(angles)[:, None, :]
    sine_table = jnp.sin(angles)[:, None, :]
    first_half = values[..., :halfway]
    second = values[..., halfway:]
    return jnp.concatenate([first_half * cosine - second * sine_table, first_half * sine_table + second * cosine], axis=-1)

def rms_scale(values, gains):
    return values * lax.rsqrt(lax.optimization_barrier(jnp.mean(values * values, axis=-1, keepdims=True)) + epsilon) * gains

def retention_step(tokens, history_length, norm_gain, w_query, w_key, w_value, w_gate, decay_rate, state, head_gain, w_out, moe_gain):
    row_count = tokens.shape[0]
    head_count = decay_rate.shape[0]
    head_width = state.shape[-1]
    inputs = tokens.astype(jnp.float32)
    normed = rms_scale(inputs, norm_gain).astype(jnp.bfloat16)

    def project(weights):
        return jnp.dot(normed, weights, preferred_element_type=jnp.float32).astype(jnp.bfloat16)
    queries = project(w_query).reshape(row_count, head_count, head_width).astype(jnp.float32)
    keys_now = project(w_key).reshape(row_count, head_count, head_width).astype(jnp.float32)
    values_now = project(w_value).reshape(row_count, head_count, head_width).astype(jnp.float32)
    gating = project(w_gate).astype(jnp.float32)
    places = history_length.astype(jnp.float32)
    queries = rotate(queries, places)
    keys_now = rotate(keys_now, places) * head_width ** (-0.5)
    retain = jnp.exp(-decay_rate)
    new_state = retain[None, :, None, None] * state + keys_now[:, :, :, None] * values_now[:, :, None, :]
    reading = jnp.einsum('bhk,bhkv->bhv', queries, new_state, precision=lax.Precision.HIGHEST)
    reading = rms_scale(reading, head_gain.reshape(head_count, head_width))
    mixed_heads = (reading.reshape(row_count, head_count * head_width) * jax.nn.silu(gating)).astype(jnp.bfloat16)
    mixed_tokens = (inputs + jnp.dot(mixed_heads, w_out, preferred_element_type=jnp.float32)).astype(jnp.bfloat16)
    normed_moe = rms_scale(mixed_tokens.astype(jnp.float32), moe_gain).astype(jnp.bfloat16)
    return (mixed_tokens, normed_moe, new_state)

def expert_apply(row_block, gate_weight, up_weight, down_weight):
    gate_part = jnp.dot(row_block, gate_weight, preferred_element_type=jnp.float32)
    up_part = jnp.dot(row_block, up_weight, preferred_element_type=jnp.float32)
    hidden = (jax.nn.silu(gate_part) * up_part).astype(jnp.bfloat16)
    return jnp.dot(hidden, down_weight, preferred_element_type=jnp.float32).astype(jnp.bfloat16)

def reference(tokens, history_length, norm_gain, w_query, w_key, w_value, w_gate, decay_rate, state, head_gain, w_out, moe_gain, route_weights, expert_group, expert_inner, expert_gate, expert_up, expert_down):
    mixed_tokens, normed_moe, new_state = retention_step(tokens, history_length, norm_gain, w_query, w_key, w_value, w_gate, decay_rate, state, head_gain, w_out, moe_gain)
    row_count = tokens.shape[0]
    experts = expert_gate.shape[0]
    per_group = experts // GROUPS
    flat_ids = (expert_group[:, None] * per_group + expert_inner).reshape(-1).astype(jnp.int32)
    slot_total = flat_ids.shape[0]
    padded_ids = jnp.concatenate([flat_ids, jnp.full((1,), -1, jnp.int32)])
    owners = jnp.concatenate([jnp.arange(slot_total, dtype=jnp.int32) // TOP_K, jnp.zeros((1,), jnp.int32)])
    scales = jnp.concatenate([route_weights.reshape(-1), jnp.zeros((1,), jnp.float32)])
    row_bound = N_EP * CAP

    def visit_expert(running, expert):
        matched = padded_ids == expert
        picked = jnp.nonzero(matched, size=row_bound, fill_value=slot_total)[0].astype(jnp.int32)
        owner_rows = owners[picked]
        weighting = jnp.where(matched[picked], scales[picked], jnp.zeros_like(scales[picked]))
        outputs = expert_apply(normed_moe[owner_rows], expert_gate[expert], expert_up[expert], expert_down[expert])
        running = running.at[owner_rows].add(outputs.astype(jnp.float32) * weighting[:, None])
        return (running, None)
    running, _ = lax.scan(visit_expert, jnp.zeros((row_count, tokens.shape[1]), jnp.float32), jnp.arange(experts, dtype=jnp.int32))
    output = (mixed_tokens.astype(jnp.float32) + running).astype(jnp.bfloat16)
    return (output, new_state)
```

```python
import jax
import jax.numpy as jnp
import numpy as np
from jax import lax
from jax.experimental import pallas as pl
from jax.experimental.pallas import tpu as pltpu
from jax.sharding import PartitionSpec as P

GROUPS = 4
TOP_K = 2


epsilon = 1e-06


BLOCK = 8


MESH = pl.DeviceIdType.MESH
STAGES = GROUPS


def dot(a, b):
    return jnp.dot(a, b, preferred_element_type=jnp.float32)


def rms(values, gains):
    mean = jnp.mean(values * values, axis=-1, keepdims=True)
    return values * lax.rsqrt(mean + epsilon) * gains


def layer_kernel(
    per_group,
    tokens,
    history_length,
    inverse,
    norm_gain,
    decay_rate,
    head_gain,
    moe_gain,
    expert_group,
    expert_inner,
    route_weights,
    query_hbm,
    key_hbm,
    value_hbm,
    gate_hbm,
    out_hbm,
    state_hbm,
    expert_gate_hbm,
    expert_up_hbm,
    expert_down_hbm,
    out,
    state,
    query_w,
    key_w,
    value_w,
    gate_w,
    out_w,
    expert_gate_w,
    expert_up_w,
    expert_down_w,
    query_columns,
    key_columns,
    value_heads,
    reading,
    meta_send,
    meta_recv,
    zsend,
    zrecv,
    hsend,
    hrecv,
    dsend,
    drecv,
    esend,
    erecv,
    osend,
    orecv,
    csend,
    crecv,
    weight_sem,
    in_sem,
    load_sem,
    meta_sems,
    z_sems,
    h_sems,
    d_sems,
    e_sems,
    o_sems,
    c_sems,
):
    device = lax.axis_index("ep")
    group = device // per_group
    inner = device % per_group
    seq_count, width = tokens.shape
    group_rows = zsend.shape[1]
    peer_rows = dsend.shape[2]
    slots = GROUPS * group_rows
    rows = per_group * peer_rows
    heads, head_width = state.shape[1], state.shape[-1]
    half = head_width // 2
    blocks = seq_count // BLOCK

    def column_peer(step):
        other = lax.rem(group + step, GROUPS)
        return other, other * per_group + inner

    def plane_peer(step):
        other = lax.rem(inner + step, per_group)
        return other, group * per_group + other

    def remote(source, target, send_sem, recv_sem, peer):
        return pltpu.make_async_remote_copy(
            src_ref=source,
            dst_ref=target,
            send_sem=send_sem,
            recv_sem=recv_sem,
            device_id=(peer,),
            device_id_type=MESH,
        )

    def column_copy(source, target, sems, step):
        other, peer = column_peer(step)
        return remote(source.at[other], target.at[step], sems.at[0, step], sems.at[1, step], peer)

    def send_home(step):
        home = lax.rem(group + GROUPS - step, GROUPS)
        return remote(
            csend.at[step],
            crecv.at[group],
            c_sems.at[0, step],
            c_sems.at[1, step],
            home * per_group + inner,
        )

    def plane_copy(source, target, sems, stage, step):
        other, peer = plane_peer(step)
        return remote(
            source.at[stage, other],
            target.at[stage, inner],
            sems.at[0, stage, step],
            sems.at[1, stage, step],
            peer,
        )

    def each_column(act):
        for step in range(1, GROUPS):
            act(step)

    def each_plane(act):
        def body(step, carry):
            act(step)
            return carry

        lax.fori_loop(1, per_group, body, 0)

    def load_all(pairs, sem):
        return [
            pltpu.make_async_copy(source, target, sem.at[index])
            for index, (source, target) in enumerate(pairs)
        ]

    weight_copies = load_all(
        (
            (key_hbm, key_w),
            (query_hbm, query_w),
            (value_hbm, value_w),
            (gate_hbm, gate_w),
            (out_hbm, out_w),
        ),
        weight_sem,
    )
    loads = load_all(
        (
            (expert_gate_hbm, expert_gate_w),
            (expert_up_hbm, expert_up_w),
            (expert_down_hbm, expert_down_w),
        ),
        load_sem,
    )

    def state_in(block):
        span = pl.ds(block * BLOCK, BLOCK)
        return pltpu.make_async_copy(state_hbm.at[span], state.at[span], in_sem.at[block])

    for copy in weight_copies[:3]:
        copy.start()
    for block in range(blocks):
        state_in(block).start()
    for copy in weight_copies[3:]:
        copy.start()
    for load in loads:
        load.start()

    barrier = pltpu.get_barrier_semaphore()

    def greet_column(step):
        pl.semaphore_signal(barrier, inc=1, device_id=(column_peer(step)[1],), device_id_type=MESH)

    def greet_plane(step):
        pl.semaphore_signal(barrier, inc=1, device_id=(plane_peer(step)[1],), device_id_type=MESH)

    each_column(greet_column)
    each_plane(greet_plane)

    square = (seq_count, seq_count)
    above = lax.broadcasted_iota(jnp.int32, square, 0)
    across = lax.broadcasted_iota(jnp.int32, square, 1)

    def column(row):
        return jnp.sum(jnp.where(above == across, row, 0.0), axis=1, keepdims=True)

    def earlier(columns, row):
        matched = sum((values == row).astype(jnp.float32) for values in columns)
        return jnp.sum(jnp.where(above < across, matched, 0.0), axis=0, keepdims=True)

    group_row = expert_group[...].astype(jnp.float32)
    inner_rows = [expert_inner[choice : choice + 1, :].astype(jnp.float32) for choice in (0, 1)]
    group_slot = group_row * group_rows + earlier([column(group_row)], group_row)
    expert_rows = [group_row * per_group + row for row in inner_rows]
    expert_columns = [column(row) for row in expert_rows]
    lanes = []
    for choice in (0, 1):
        slot = earlier(expert_columns, expert_rows[choice])
        lanes.append(column(inner_rows[choice] * peer_rows + slot + 1.0))
    for choice in (0, 1):
        weight = column(route_weights[choice : choice + 1, :])
        high = weight.astype(jnp.bfloat16).astype(jnp.float32)
        lanes += [high, weight - high]
    lane = lax.broadcasted_iota(jnp.int32, (seq_count, meta_send.shape[-1]), 1)
    token_meta = jnp.zeros(lane.shape, jnp.float32)
    for index, value in enumerate(lanes):
        token_meta = jnp.where(lane == index, value, token_meta)
    slot_above = lax.broadcasted_iota(jnp.int32, (slots, seq_count), 0).astype(jnp.float32)
    slot_across = lax.broadcasted_iota(jnp.int32, (seq_count, slots), 1).astype(jnp.float32)
    placing = (slot_above == group_slot).astype(jnp.float32).astype(jnp.bfloat16)
    collecting = (slot_across == column(group_slot)).astype(jnp.float32).astype(jnp.bfloat16)
    meta = dot(placing, token_meta.astype(jnp.bfloat16)).astype(jnp.bfloat16)
    meta_send[...] = meta.reshape(meta_send.shape)
    zsend[...] = dot(placing, tokens[...]).astype(jnp.bfloat16).reshape(zsend.shape)
    pl.semaphore_wait(barrier, GROUPS - 1 + per_group - 1)
    each_column(lambda step: column_copy(meta_send, meta_recv, meta_sems, step).start())
    each_column(lambda step: column_copy(zsend, zrecv, z_sems, step).start())
    meta_recv[0] = meta_send[group]
    zrecv[0] = zsend[group]
    picks_of = {}
    weights_of = {}

    def route(stage):
        if stage:
            column_copy(meta_send, meta_recv, meta_sems, stage).wait_recv()
        meta = meta_recv[stage].astype(jnp.float32)
        row_ids = lax.broadcasted_iota(jnp.int32, (group_rows, rows), 1).astype(jnp.float32) + 1.0
        first = (row_ids == meta[:, 0:1]).astype(jnp.float32)
        second = (row_ids == meta[:, 1:2]).astype(jnp.float32)
        weights = first * (meta[:, 2:3] + meta[:, 3:4]) + second * (meta[:, 4:5] + meta[:, 5:6])
        high = weights.astype(jnp.bfloat16)
        picks_of[stage] = (first + second).astype(jnp.bfloat16)
        weights_of[stage] = (high, (weights - high.astype(jnp.float32)).astype(jnp.bfloat16))

    def spread(stage, received, sent, landed, sems):
        block = lax.dot_general(
            picks_of[stage],
            received[stage],
            (((0,), (0,)), ((), ())),
            preferred_element_type=jnp.float32,
        ).astype(jnp.bfloat16)
        sent[stage] = block.reshape(sent.shape[1:])
        each_plane(lambda step: plane_copy(sent, landed, sems, stage, step).start())
        landed[stage, inner] = sent[stage, inner]

    def spread_tokens(stage):
        route(stage)
        if stage:
            column_copy(zsend, zrecv, z_sems, stage).wait_recv()
        spread(stage, zrecv, dsend, drecv, d_sems)

    def spread_heads(stage):
        if stage:
            column_copy(hsend, hrecv, h_sems, stage).wait_recv()
        spread(stage, hrecv, esend, erecv, e_sems)

    spread_tokens(0)

    inputs = tokens[...].astype(jnp.float32)
    normed = rms(inputs, norm_gain[...]).astype(jnp.bfloat16)
    places = column(history_length[...].astype(jnp.float32))
    angles = places * inverse[...]
    cosine, sine = jnp.cos(angles), jnp.sin(angles)
    cosines = jnp.concatenate([cosine] * (2 * heads), axis=1)
    sines = jnp.concatenate([-sine, sine] * heads, axis=1)
    head_lane = lax.broadcasted_iota(jnp.int32, cosines.shape, 1)
    leading = lax.rem(head_lane, head_width) < half

    def rounded(weights):
        return dot(normed, weights[...]).astype(jnp.bfloat16).astype(jnp.float32)

    def rotated(values):
        partner = jnp.where(
            leading, jnp.roll(values, -half, axis=1), jnp.roll(values, half, axis=1)
        )
        return values * cosines + partner * sines

    weight_copies[0].wait()
    keys = rotated(rounded(key_w)) * head_width ** (-0.5)
    weight_copies[1].wait()
    queries = rotated(rounded(query_w))
    for block in range(blocks):
        span = slice(block * BLOCK, (block + 1) * BLOCK)
        key_columns[block] = keys[span].T
        query_columns[block] = queries[span].T
    weight_copies[2].wait()
    values = rounded(value_w)
    for head in range(heads):
        value_heads[head] = values[:, head * head_width : (head + 1) * head_width]
    retain = [
        jnp.exp(jnp.full((1, head_width), -decay_rate[head], jnp.float32)) for head in range(heads)
    ]

    def update(block, carry):
        state_in(block).wait()
        for head in range(heads):
            span = slice(head * head_width, (head + 1) * head_width)
            block_values = value_heads[head, pl.ds(block * BLOCK, BLOCK), :]
            block_keys = key_columns[block, span, :]
            block_queries = query_columns[block, span, :]
            read_rows = []
            for index in range(BLOCK):
                sequence = block * BLOCK + index
                fresh = (
                    retain[head] * state[sequence, head]
                    + block_keys[:, index : index + 1] * block_values[index : index + 1, :]
                )
                state[sequence, head] = fresh
                read_rows.append(
                    jnp.sum(block_queries[:, index : index + 1] * fresh, axis=0, keepdims=True)
                )
            reading[head, pl.ds(block * BLOCK, BLOCK), :] = jnp.concatenate(read_rows, axis=0)
        return carry

    lax.fori_loop(0, blocks // 2, update, 0)
    spread_tokens(1)
    lax.fori_loop(blocks // 2, blocks, update, 0)
    weight_copies[3].wait()
    gating = rounded(gate_w)
    read = jnp.concatenate(
        [
            rms(
                reading[head],
                head_gain[:, head * head_width : (head + 1) * head_width],
            )
            for head in range(heads)
        ],
        axis=1,
    )
    mixed_heads = (read * jax.nn.silu(gating)).astype(jnp.bfloat16)
    hsend[...] = dot(placing, mixed_heads).astype(jnp.bfloat16).reshape(hsend.shape)
    each_column(lambda step: column_copy(hsend, hrecv, h_sems, step).start())
    hrecv[0] = hsend[group]
    spread_heads(0)
    spread_tokens(2)
    spread_tokens(3)
    weight_copies[4].wait()
    mixed = (inputs + dot(mixed_heads, out_w[...])).astype(jnp.bfloat16)
    for stage in range(1, STAGES):
        spread_heads(stage)
    for load in loads:
        load.wait()

    def run_expert(stage):
        each_plane(lambda step: plane_copy(dsend, drecv, d_sems, stage, step).wait_recv())
        each_plane(lambda step: plane_copy(esend, erecv, e_sems, stage, step).wait_recv())
        token_rows = drecv[stage].reshape(rows, width).astype(jnp.float32)
        head_rows = erecv[stage].reshape(rows, erecv.shape[-1])
        block = (token_rows + dot(head_rows, out_w[...])).astype(jnp.bfloat16)
        block = rms(block.astype(jnp.float32), moe_gain[...]).astype(jnp.bfloat16)
        hidden = jax.nn.silu(dot(block, expert_gate_w[...])) * dot(block, expert_up_w[...])
        block = dot(hidden.astype(jnp.bfloat16), expert_down_w[...]).astype(jnp.bfloat16)
        osend[stage] = block.reshape(osend.shape[1:])

    def send_back(stage):
        each_plane(lambda step: plane_copy(osend, orecv, o_sems, stage, step).start())
        orecv[stage, inner] = osend[stage, inner]

    def combine(stage):
        each_plane(lambda step: plane_copy(osend, orecv, o_sems, stage, step).wait_recv())
        block = orecv[stage].reshape(rows, width)
        high, low = weights_of[stage]
        csend[stage] = (dot(high, block) + dot(low, block)).astype(jnp.bfloat16)
        if stage:
            send_home(stage).start()
        else:
            crecv[group] = csend[0]

    run_expert(0)
    run_expert(1)
    send_back(1)
    run_expert(2)
    send_back(2)
    run_expert(3)
    send_back(3)
    send_back(0)
    combine(1)
    combine(2)
    combine(3)
    combine(0)
    each_column(lambda step: send_home(step).wait_recv())
    block = dot(collecting, crecv[...].reshape(slots, width))
    out[...] = (mixed.astype(jnp.float32) + block).astype(jnp.bfloat16)
    each_column(lambda step: column_copy(meta_send, meta_recv, meta_sems, step).wait_send())
    each_column(lambda step: column_copy(zsend, zrecv, z_sems, step).wait_send())
    each_column(lambda step: column_copy(hsend, hrecv, h_sems, step).wait_send())
    each_column(lambda step: send_home(step).wait_send())

    def drain(stage, carry):
        each_plane(lambda step: plane_copy(dsend, drecv, d_sems, stage, step).wait_send())
        each_plane(lambda step: plane_copy(esend, erecv, e_sems, stage, step).wait_send())
        each_plane(lambda step: plane_copy(osend, orecv, o_sems, stage, step).wait_send())
        return carry

    lax.fori_loop(0, STAGES, drain, 0)


def local(
    tokens,
    history_length,
    norm_gain,
    w_query,
    w_key,
    w_value,
    w_gate,
    decay_rate,
    state,
    head_gain,
    w_out,
    moe_gain,
    route_weights,
    expert_group,
    expert_inner,
    expert_gate,
    expert_up,
    expert_down,
):
    experts = lax.axis_size("ep")
    per_group = experts // GROUPS
    heads = decay_rate.shape[0]
    seq_count, model_width = tokens.shape
    head_width = state.shape[-1]
    mixed_width = heads * head_width
    half = head_width // 2
    blocks = seq_count // BLOCK
    inverse = (10000.0 ** (-np.arange(half) / half)).astype(np.float32)
    capacity = max(2, 4 * seq_count // experts)
    group_rows = -(-min(seq_count, per_group * capacity // TOP_K) // 8) * 8
    peer_rows = -(-capacity // 8) * 8
    vmem = pl.BlockSpec(memory_space=pltpu.VMEM)
    smem = pl.BlockSpec(memory_space=pltpu.SMEM)
    hbm = pl.BlockSpec(memory_space=pl.ANY)
    dma = pltpu.SemaphoreType.DMA
    bf16, f32 = jnp.bfloat16, jnp.float32

    def column_buffer(lanes):
        return [pltpu.VMEM((GROUPS, group_rows, lanes), bf16)] * 2

    def plane_buffer(lanes):
        return [pltpu.VMEM((STAGES, per_group, peer_rows, lanes), bf16)] * 2

    weights = (w_query, w_key, w_value, w_gate, w_out, expert_gate[0], expert_up[0], expert_down[0])
    state_bytes = state.size // head_width * max(head_width, 128) * 4

    def kernel(*refs):
        layer_kernel(per_group, *refs)

    output, new_state = pl.pallas_call(
        kernel,
        name="layer",
        out_shape=(
            jax.ShapeDtypeStruct((seq_count, model_width), bf16),
            pltpu.VMEM(state.shape, f32),
        ),
        in_specs=[vmem] * 4 + [smem] + [vmem] * 5 + [hbm] * 9,
        out_specs=(vmem, vmem),
        scratch_shapes=[pltpu.VMEM(weight.shape, bf16) for weight in weights]
        + [
            pltpu.VMEM((blocks, mixed_width, BLOCK), f32),
            pltpu.VMEM((blocks, mixed_width, BLOCK), f32),
            pltpu.VMEM((heads, seq_count, head_width), f32),
            pltpu.VMEM((heads, seq_count, head_width), f32),
        ]
        + column_buffer(128)
        + column_buffer(model_width)
        + column_buffer(mixed_width)
        + plane_buffer(model_width)
        + plane_buffer(mixed_width)
        + plane_buffer(model_width)
        + column_buffer(model_width)
        + [
            dma((5,)),
            dma((blocks,)),
            dma((3,)),
            dma((2, GROUPS)),
            dma((2, GROUPS)),
            dma((2, GROUPS)),
            dma((2, STAGES, per_group)),
            dma((2, STAGES, per_group)),
            dma((2, STAGES, per_group)),
            dma((2, STAGES)),
        ],
        compiler_params=pltpu.CompilerParams(
            collective_id=0,
            has_side_effects=True,
            vmem_limit_bytes=63 * 1024 * 1024 - state_bytes,
        ),
    )(
        tokens,
        history_length.reshape(1, -1),
        inverse.reshape(1, -1),
        norm_gain.reshape(1, -1),
        decay_rate,
        head_gain.reshape(1, -1),
        moe_gain.reshape(1, -1),
        expert_group.reshape(1, -1),
        expert_inner.T,
        route_weights.T,
        w_query,
        w_key,
        w_value,
        w_gate,
        w_out,
        state,
        expert_gate[0],
        expert_up[0],
        expert_down[0],
    )
    return (output, new_state)


def solution(mesh):
    return jax.shard_map(
        local,
        mesh=mesh,
        in_specs=(
            P("ep", None),
            P("ep"),
            P(),
            P(),
            P(),
            P(),
            P(),
            P(),
            P("ep", None, None, None),
            P(),
            P(),
            P(),
            P("ep", None),
            P("ep"),
            P("ep", None),
            P("ep", None, None),
            P("ep", None, None),
            P("ep", None, None),
        ),
        out_specs=(P("ep", None), P("ep", None, None, None)),
        check_vma=False,
    )
```

```python
import jax
import jax.numpy as jnp
import numpy as np
from jax import lax
from jax.experimental import pallas as pl
from jax.experimental.pallas import tpu as pltpu
from jax.sharding import PartitionSpec as P

GROUPS = 4
TOP_K = 2


epsilon = 1e-06


BLOCK = 8


MESH = pl.DeviceIdType.MESH
STAGES = GROUPS
QUARTERS = 4
ORDER = (2, 1, 3)


def dot(a, b):
    return jnp.dot(a, b, preferred_element_type=jnp.float32)


def rms(values, gains):
    mean = jnp.mean(values * values, axis=-1, keepdims=True)
    return values * lax.rsqrt(mean + epsilon) * gains


def layer_kernel(
    per_group,
    capacity,
    tokens,
    history_length,
    inverse,
    norm_gain,
    decay_rate,
    head_gain,
    moe_gain,
    expert_group,
    expert_inner,
    route_weights,
    query_hbm,
    key_hbm,
    value_hbm,
    gate_hbm,
    out_hbm,
    state_hbm,
    expert_gate_hbm,
    expert_up_hbm,
    expert_down_hbm,
    out,
    state,
    query_w,
    key_w,
    value_w,
    gate_w,
    out_w,
    expert_gate_w,
    expert_up_w,
    expert_down_w,
    query_columns,
    key_columns,
    value_heads,
    reading,
    overlap,
    meta_send,
    meta_recv,
    zsend,
    zrecv,
    hsend,
    hrecv,
    dsend,
    drecv,
    esend,
    erecv,
    osend,
    orecv,
    csend,
    crecv,
    weight_sem,
    in_sem,
    load_sem,
    meta_sems,
    z_sems,
    h_sems,
    d_sems,
    e_sems,
    o_sems,
    c_sems,
):
    device = lax.axis_index("ep")
    group = device // per_group
    inner = device % per_group
    seq_count, width = tokens.shape
    group_rows = zsend.shape[1]
    slots = GROUPS * group_rows
    rows = per_group * capacity
    tiles = per_group * BLOCK
    parts = capacity * QUARTERS // BLOCK
    heads, head_width = state.shape[1], state.shape[-1]
    half = head_width // 2
    blocks = seq_count // BLOCK

    def column_peer(step):
        other = lax.rem(group + step, GROUPS)
        return other, other * per_group + inner

    def plane_peer(step):
        other = lax.rem(inner + step, per_group)
        return other, group * per_group + other

    def remote(source, target, send_sem, recv_sem, peer):
        return pltpu.make_async_remote_copy(
            src_ref=source,
            dst_ref=target,
            send_sem=send_sem,
            recv_sem=recv_sem,
            device_id=(peer,),
            device_id_type=MESH,
        )

    def column_copy(source, target, sems, step):
        other, peer = column_peer(step)
        return remote(source.at[other], target.at[step], sems.at[0, step], sems.at[1, step], peer)

    def send_home(step):
        home = lax.rem(group + GROUPS - step, GROUPS)
        return remote(
            csend.at[step],
            crecv.at[group],
            c_sems.at[0, step],
            c_sems.at[1, step],
            home * per_group + inner,
        )

    def plane_copy(source, target, sems, stage, step):
        other, peer = plane_peer(step)
        return remote(
            source.at[stage, other],
            target.at[stage, inner],
            sems.at[0, stage],
            sems.at[1, stage],
            peer,
        )

    def plane_total(source, target, sems, stage):
        others = pl.ds(0, per_group - 1)
        return remote(
            source.at[stage, others],
            target.at[stage, others],
            sems.at[0, stage],
            sems.at[1, stage],
            plane_peer(1)[1],
        )

    def each_column(act):
        for step in ORDER:
            act(step)

    def each_plane(act):
        def body(step, carry):
            act(step)
            return carry

        lax.fori_loop(1, per_group, body, 0)

    def load_all(pairs, sem):
        return [
            pltpu.make_async_copy(source, target, sem.at[index])
            for index, (source, target) in enumerate(pairs)
        ]

    weight_copies = load_all(
        (
            (key_hbm, key_w),
            (query_hbm, query_w),
            (value_hbm, value_w),
            (gate_hbm, gate_w),
            (out_hbm, out_w),
        ),
        weight_sem,
    )
    loads = load_all(
        (
            (expert_gate_hbm, expert_gate_w),
            (expert_up_hbm, expert_up_w),
            (expert_down_hbm, expert_down_w),
        ),
        load_sem,
    )

    def state_in(block):
        span = pl.ds(block * BLOCK, BLOCK)
        return pltpu.make_async_copy(state_hbm.at[span], state.at[span], in_sem.at[block])

    for copy in weight_copies[:3]:
        copy.start()
    for block in range(blocks):
        state_in(block).start()
    for copy in weight_copies[3:]:
        copy.start()
    for load in loads:
        load.start()

    barrier = pltpu.get_barrier_semaphore()

    def greet_column(step):
        pl.semaphore_signal(barrier, inc=1, device_id=(column_peer(step)[1],), device_id_type=MESH)

    def greet_plane(step):
        pl.semaphore_signal(barrier, inc=1, device_id=(plane_peer(step)[1],), device_id_type=MESH)

    each_column(greet_column)
    each_plane(greet_plane)

    square = (seq_count, seq_count)
    above = lax.broadcasted_iota(jnp.int32, square, 0)
    across = lax.broadcasted_iota(jnp.int32, square, 1)

    def column(row):
        return jnp.sum(jnp.where(above == across, row, 0.0), axis=1, keepdims=True)

    def earlier(columns, row):
        matched = sum((values == row).astype(jnp.float32) for values in columns)
        return jnp.sum(jnp.where(above < across, matched, 0.0), axis=0, keepdims=True)

    group_row = expert_group[...].astype(jnp.float32)
    inner_rows = [expert_inner[choice : choice + 1, :].astype(jnp.float32) for choice in (0, 1)]
    group_slot = group_row * group_rows + earlier([column(group_row)], group_row)
    expert_rows = [group_row * per_group + row for row in inner_rows]
    expert_columns = [column(row) for row in expert_rows]
    lanes = []
    for choice in (0, 1):
        slot = earlier(expert_columns, expert_rows[choice])
        lanes.append(column(inner_rows[choice] * capacity + slot + 1.0))
    for choice in (0, 1):
        weight = column(route_weights[choice : choice + 1, :])
        high = weight.astype(jnp.bfloat16).astype(jnp.float32)
        lanes += [high, weight - high]
    lane = lax.broadcasted_iota(jnp.int32, (seq_count, meta_send.shape[-1]), 1)
    token_meta = jnp.zeros(lane.shape, jnp.float32)
    for index, value in enumerate(lanes):
        token_meta = jnp.where(lane == index, value, token_meta)
    slot_above = lax.broadcasted_iota(jnp.int32, (slots, seq_count), 0).astype(jnp.float32)
    slot_across = lax.broadcasted_iota(jnp.int32, (seq_count, slots), 1).astype(jnp.float32)
    placing = (slot_above == group_slot).astype(jnp.float32).astype(jnp.bfloat16)
    collecting = (slot_across == column(group_slot)).astype(jnp.float32).astype(jnp.bfloat16)
    meta = dot(placing, token_meta.astype(jnp.bfloat16)).astype(jnp.bfloat16)
    meta_send[...] = meta.reshape(meta_send.shape)
    zsend[...] = dot(placing, tokens[...]).astype(jnp.bfloat16).reshape(zsend.shape)
    with jax.named_scope("barrier"):
        pl.semaphore_wait(barrier, GROUPS - 1 + per_group - 1)
    each_column(lambda step: column_copy(meta_send, meta_recv, meta_sems, step).start())
    each_column(lambda step: column_copy(zsend, zrecv, z_sems, step).start())
    meta_recv[0] = meta_send[group]
    zrecv[0] = zsend[group]
    def packed_places(shape, axis):
        index = lax.broadcasted_iota(jnp.int32, shape, axis)
        part = sum((index >= tiles * bound).astype(jnp.int32) for bound in range(1, parts))
        index = index - part * tiles
        place = (index & (BLOCK - 1)) * parts + part
        return (index >> 3) * capacity + (place >> 2), place & (QUARTERS - 1)

    packed_rows, packed_quarter = packed_places((1, parts * tiles), 1)
    row_names = packed_rows.astype(jnp.float32) + 1.0
    in_quarter = [(packed_quarter == part).astype(jnp.float32) for part in range(QUARTERS)]
    row_number = lax.broadcasted_iota(jnp.int32, (rows, parts * tiles), 0)
    same_row = (row_number == packed_rows).astype(jnp.float32)
    packing = jnp.concatenate([same_row * part for part in in_quarter], axis=0).astype(jnp.bfloat16)
    picks_of = {}
    weights_of = {}

    def stacked(block):
        share = block.shape[-1] // QUARTERS
        return jnp.concatenate(
            [block[:, part * share : (part + 1) * share] for part in range(QUARTERS)], axis=0
        )

    def unstacked(block):
        share = block.shape[0] // QUARTERS
        return jnp.concatenate(
            [block[part * share : (part + 1) * share] for part in range(QUARTERS)], axis=1
        )

    def take(picks, block):
        return lax.dot_general(
            picks, block, (((0,), (0,)), ((), ())), preferred_element_type=jnp.float32
        ).astype(jnp.bfloat16)

    def store_packed(sent, stage, block):
        share = block.shape[-1]
        for part in range(parts):
            sent[stage, :, :, part * share : (part + 1) * share] = block[
                part * tiles : (part + 1) * tiles
            ].reshape(per_group, BLOCK, share)

    def load_packed(landed, stage):
        block = landed[stage].reshape(tiles, landed.shape[-1])
        share = block.shape[-1] // parts
        return jnp.concatenate(
            [block[:, part * share : (part + 1) * share] for part in range(parts)], axis=0
        )

    def route(stage):
        if stage:
            column_copy(meta_send, meta_recv, meta_sems, stage).wait_recv()
        meta = meta_recv[stage].astype(jnp.float32)
        first = (row_names == meta[:, 0:1]).astype(jnp.float32)
        second = (row_names == meta[:, 1:2]).astype(jnp.float32)
        weights = first * (meta[:, 2:3] + meta[:, 3:4]) + second * (meta[:, 4:5] + meta[:, 5:6])
        both = first + second
        picks = jnp.concatenate([both * part for part in in_quarter], axis=0)
        weights = jnp.concatenate([weights * part for part in in_quarter], axis=0)
        high = weights.astype(jnp.bfloat16)
        picks_of[stage] = picks.astype(jnp.bfloat16)
        weights_of[stage] = (high, (weights - high.astype(jnp.float32)).astype(jnp.bfloat16))

    def spread(stage, received, sent, landed, sems):
        block = stacked(received[stage].astype(jnp.float32)).astype(jnp.bfloat16)
        store_packed(sent, stage, take(picks_of[stage], block))
        each_plane(lambda step: plane_copy(sent, landed, sems, stage, step).start())
        landed[stage, inner] = sent[stage, inner]

    def spread_tokens(stage):
        route(stage)
        if stage:
            column_copy(zsend, zrecv, z_sems, stage).wait_recv()
        spread(stage, zrecv, dsend, drecv, d_sems)

    def spread_heads(stage):
        if stage:
            column_copy(hsend, hrecv, h_sems, stage).wait_recv()
        spread(stage, hrecv, esend, erecv, e_sems)

    with jax.named_scope("spread_tokens_0"):
        spread_tokens(0)

    inputs = tokens[...].astype(jnp.float32)
    normed = rms(inputs, norm_gain[...]).astype(jnp.bfloat16)
    places = column(history_length[...].astype(jnp.float32))
    angles = places * inverse[...]
    cosine, sine = jnp.cos(angles), jnp.sin(angles)
    cosines = jnp.concatenate([cosine] * (2 * heads), axis=1)
    sines = jnp.concatenate([-sine, sine] * heads, axis=1)
    head_lane = lax.broadcasted_iota(jnp.int32, cosines.shape, 1)
    leading = lax.rem(head_lane, head_width) < half

    def rounded(weights):
        return dot(normed, weights[...]).astype(jnp.bfloat16).astype(jnp.float32)

    def rotated(values):
        partner = jnp.where(
            leading, jnp.roll(values, -half, axis=1), jnp.roll(values, half, axis=1)
        )
        return values * cosines + partner * sines

    with jax.named_scope("wait_k"):
        weight_copies[0].wait()
    keys = rotated(rounded(key_w)) * head_width ** (-0.5)
    with jax.named_scope("wait_q"):
        weight_copies[1].wait()
    queries = rotated(rounded(query_w))
    for block in range(blocks):
        span = slice(block * BLOCK, (block + 1) * BLOCK)
        key_columns[block] = keys[span].T
        query_columns[block] = queries[span].T
    with jax.named_scope("wait_v"):
        weight_copies[2].wait()
    values = rounded(value_w)
    for head in range(heads):
        value_heads[head] = values[:, head * head_width : (head + 1) * head_width]
    retain = [
        jnp.exp(jnp.full((1, head_width), -decay_rate[head], jnp.float32)) for head in range(heads)
    ]

    products = keys * queries
    for head in range(heads):
        span = slice(head * head_width, (head + 1) * head_width)
        overlap[head] = jnp.sum(products[:, span], axis=1, keepdims=True)

    def read(block, carry):
        state_in(block).wait()
        span = pl.ds(block * BLOCK, BLOCK)
        for head in range(heads):
            lanes = slice(head * head_width, (head + 1) * head_width)
            block_queries = query_columns[block, lanes, :]
            read_rows = [
                jnp.sum(
                    block_queries[:, index : index + 1] * state[block * BLOCK + index, head],
                    axis=0,
                    keepdims=True,
                )
                for index in range(BLOCK)
            ]
            reading[head, span, :] = (
                retain[head] * jnp.concatenate(read_rows, axis=0)
                + overlap[head, span, :] * value_heads[head, span, :]
            )
        return carry

    def update(block, carry):
        span = pl.ds(block * BLOCK, BLOCK)
        for head in range(heads):
            lanes = slice(head * head_width, (head + 1) * head_width)
            block_values = value_heads[head, span, :]
            block_keys = key_columns[block, lanes, :]
            for index in range(BLOCK):
                sequence = block * BLOCK + index
                state[sequence, head] = (
                    retain[head] * state[sequence, head]
                    + block_keys[:, index : index + 1] * block_values[index : index + 1, :]
                )
        return carry

    def advance(first, last):
        with jax.named_scope(f"advance_{first}"):
            lax.fori_loop(first, last, update, 0)

    with jax.named_scope("read_a"):
        lax.fori_loop(0, 2 * blocks // 3, read, 0)
    with jax.named_scope("spread_tokens_2"):
        spread_tokens(2)
    with jax.named_scope("read_b"):
        lax.fori_loop(2 * blocks // 3, blocks, read, 0)
    with jax.named_scope("spread_tokens_1"):
        spread_tokens(1)
    with jax.named_scope("wait_g"):
        weight_copies[3].wait()
    gating = rounded(gate_w)
    read_heads = jnp.concatenate(
        [
            rms(
                reading[head],
                head_gain[:, head * head_width : (head + 1) * head_width],
            )
            for head in range(heads)
        ],
        axis=1,
    )
    mixed_heads = (read_heads * jax.nn.silu(gating)).astype(jnp.bfloat16)
    hsend[...] = dot(placing, mixed_heads).astype(jnp.bfloat16).reshape(hsend.shape)
    each_column(lambda step: column_copy(hsend, hrecv, h_sems, step).start())
    hrecv[0] = hsend[group]
    with jax.named_scope("spread_heads_0"):
        spread_heads(0)
    with jax.named_scope("spread_tokens_3"):
        spread_tokens(3)
    for stage in ORDER:
        with jax.named_scope(f"spread_heads_{stage}"):
            spread_heads(stage)
    with jax.named_scope("wait_oe"):
        weight_copies[4].wait()
        for load in loads:
            load.wait()

    def run_expert(stage):
        plane_total(dsend, drecv, d_sems, stage).wait_recv()
        plane_total(esend, erecv, e_sems, stage).wait_recv()
        token_rows = unstacked(dot(packing, load_packed(drecv, stage)))
        head_rows = unstacked(dot(packing, load_packed(erecv, stage))).astype(jnp.bfloat16)
        block = (token_rows + dot(head_rows, out_w[...])).astype(jnp.bfloat16)
        block = rms(block.astype(jnp.float32), moe_gain[...]).astype(jnp.bfloat16)
        hidden = jax.nn.silu(dot(block, expert_gate_w[...])) * dot(block, expert_up_w[...])
        block = dot(hidden.astype(jnp.bfloat16), expert_down_w[...]).astype(jnp.bfloat16)
        store_packed(osend, stage, take(packing, stacked(block)))

    def send_back(stage):
        each_plane(lambda step: plane_copy(osend, orecv, o_sems, stage, step).start())
        orecv[stage, inner] = osend[stage, inner]

    def combine(stage):
        plane_total(osend, orecv, o_sems, stage).wait_recv()
        block = load_packed(orecv, stage)
        high, low = weights_of[stage]
        csend[stage] = unstacked(dot(high, block) + dot(low, block)).astype(jnp.bfloat16)
        if stage:
            send_home(stage).start()
        else:
            crecv[group] = csend[0]

    advance(0, blocks // 6)
    with jax.named_scope("run_expert_0"):
        run_expert(0)
    for stage in ORDER:
        with jax.named_scope(f"run_expert_{stage}"):
            run_expert(stage)
        send_back(stage)
    send_back(0)
    advance(blocks // 6, blocks // 2)
    for place, stage in enumerate(ORDER):
        with jax.named_scope(f"combine_{stage}"):
            combine(stage)
        advance((3 + place) * blocks // 6, (4 + place) * blocks // 6)
    with jax.named_scope("combine_0"):
        combine(0)
    with jax.named_scope("mixed"):
        mixed = (inputs + dot(mixed_heads, out_w[...])).astype(jnp.bfloat16)
    with jax.named_scope("wait_home"):
        each_column(lambda step: send_home(step).wait_recv())
    block = dot(collecting, crecv[...].reshape(slots, width))
    out[...] = (mixed.astype(jnp.float32) + block).astype(jnp.bfloat16)
    each_column(lambda step: column_copy(meta_send, meta_recv, meta_sems, step).wait_send())
    each_column(lambda step: column_copy(zsend, zrecv, z_sems, step).wait_send())
    each_column(lambda step: column_copy(hsend, hrecv, h_sems, step).wait_send())
    each_column(lambda step: send_home(step).wait_send())

    for stage in range(STAGES):
        plane_total(dsend, drecv, d_sems, stage).wait_send()
        plane_total(esend, erecv, e_sems, stage).wait_send()
        plane_total(osend, orecv, o_sems, stage).wait_send()


def finish_kernel(output, state, out, state_out, sem):
    blocks = sem.shape[0] - 1
    share = state.shape[0] // blocks
    copies = [pltpu.make_async_copy(output, out, sem.at[blocks])]
    for block in range(blocks):
        span = pl.ds(block * share, share)
        copies.append(pltpu.make_async_copy(state.at[span], state_out.at[span], sem.at[block]))
    for copy in copies:
        copy.start()
    for copy in copies:
        copy.wait()


def finish(output, new_state):
    vmem = pl.BlockSpec(memory_space=pltpu.VMEM)
    hbm = pl.BlockSpec(memory_space=pl.ANY)
    return pl.pallas_call(
        finish_kernel,
        name="finish",
        out_shape=(
            jax.ShapeDtypeStruct(output.shape, output.dtype),
            jax.ShapeDtypeStruct(new_state.shape, new_state.dtype),
        ),
        in_specs=[vmem, vmem],
        out_specs=(hbm, hbm),
        scratch_shapes=[pltpu.SemaphoreType.DMA((2 * new_state.shape[0] // BLOCK + 1,))],
        compiler_params=pltpu.CompilerParams(vmem_limit_bytes=4 * 1024 * 1024),
    )(output, new_state)


def local(
    tokens,
    history_length,
    norm_gain,
    w_query,
    w_key,
    w_value,
    w_gate,
    decay_rate,
    state,
    head_gain,
    w_out,
    moe_gain,
    route_weights,
    expert_group,
    expert_inner,
    expert_gate,
    expert_up,
    expert_down,
):
    experts = lax.axis_size("ep")
    per_group = experts // GROUPS
    heads = decay_rate.shape[0]
    seq_count, model_width = tokens.shape
    head_width = state.shape[-1]
    mixed_width = heads * head_width
    half = head_width // 2
    blocks = seq_count // BLOCK
    inverse = (10000.0 ** (-np.arange(half) / half)).astype(np.float32)
    capacity = max(2, 4 * seq_count // experts)
    group_rows = -(-min(seq_count, per_group * capacity // TOP_K) // 8) * 8
    capacity += capacity % 2
    packed = capacity * QUARTERS // BLOCK
    vmem = pl.BlockSpec(memory_space=pltpu.VMEM)
    smem = pl.BlockSpec(memory_space=pltpu.SMEM)
    hbm = pl.BlockSpec(memory_space=pl.ANY)
    dma = pltpu.SemaphoreType.DMA
    bf16, f32 = jnp.bfloat16, jnp.float32

    def column_buffer(lanes):
        return [pltpu.VMEM((GROUPS, group_rows, lanes), bf16)] * 2

    def plane_buffer(lanes):
        return [pltpu.VMEM((STAGES, per_group, BLOCK, lanes * packed // QUARTERS), bf16)] * 2

    weights = (w_query, w_key, w_value, w_gate, w_out, expert_gate[0], expert_up[0], expert_down[0])
    state_bytes = state.size // head_width * max(head_width, 128) * 4

    def kernel(*refs):
        layer_kernel(per_group, capacity, *refs)

    output, new_state = pl.pallas_call(
        kernel,
        name="layer",
        out_shape=(
            pltpu.VMEM((seq_count, model_width), bf16),
            pltpu.VMEM(state.shape, f32),
        ),
        in_specs=[vmem] * 4 + [smem] + [vmem] * 5 + [hbm] * 9,
        out_specs=(vmem, vmem),
        scratch_shapes=[pltpu.VMEM(weight.shape, bf16) for weight in weights]
        + [
            pltpu.VMEM((blocks, mixed_width, BLOCK), f32),
            pltpu.VMEM((blocks, mixed_width, BLOCK), f32),
            pltpu.VMEM((heads, seq_count, head_width), f32),
            pltpu.VMEM((heads, seq_count, head_width), f32),
            pltpu.VMEM((heads, seq_count, 1), f32),
        ]
        + column_buffer(128)
        + column_buffer(model_width)
        + column_buffer(mixed_width)
        + plane_buffer(model_width)
        + plane_buffer(mixed_width)
        + plane_buffer(model_width)
        + column_buffer(model_width)
        + [
            dma((5,)),
            dma((blocks,)),
            dma((3,)),
            dma((2, GROUPS)),
            dma((2, GROUPS)),
            dma((2, GROUPS)),
            dma((2, STAGES)),
            dma((2, STAGES)),
            dma((2, STAGES)),
            dma((2, STAGES)),
        ],
        compiler_params=pltpu.CompilerParams(
            collective_id=0,
            has_side_effects=True,
            vmem_limit_bytes=63 * 1024 * 1024 - state_bytes,
        ),
    )(
        tokens,
        history_length.reshape(1, -1),
        inverse.reshape(1, -1),
        norm_gain.reshape(1, -1),
        decay_rate,
        head_gain.reshape(1, -1),
        moe_gain.reshape(1, -1),
        expert_group.reshape(1, -1),
        expert_inner.T,
        route_weights.T,
        w_query,
        w_key,
        w_value,
        w_gate,
        w_out,
        state,
        expert_gate[0],
        expert_up[0],
        expert_down[0],
    )
    return finish(output, new_state)


def solution(mesh):
    return jax.shard_map(
        local,
        mesh=mesh,
        in_specs=(
            P("ep", None),
            P("ep"),
            P(),
            P(),
            P(),
            P(),
            P(),
            P(),
            P("ep", None, None, None),
            P(),
            P(),
            P(),
            P("ep", None),
            P("ep"),
            P("ep", None),
            P("ep", None, None),
            P("ep", None, None),
            P("ep", None, None),
        ),
        out_specs=(P("ep", None), P("ep", None, None, None)),
        check_vma=False,
    )
```

```python
import jax
import jax.numpy as jnp
import numpy as np
from jax import lax
from jax.experimental import pallas as pl
from jax.experimental.pallas import tpu as pltpu
from jax.sharding import PartitionSpec as P

GROUPS = 4
TOP_K = 2


epsilon = 1e-06


BLOCK = 8


MESH = pl.DeviceIdType.MESH
STAGES = GROUPS
QUARTERS = 4
ORDER = (2, 1, 3)


def dot(a, b):
    return jnp.dot(a, b, preferred_element_type=jnp.float32)


def rms(values, gains):
    mean = jnp.mean(values * values, axis=-1, keepdims=True)
    return values * lax.rsqrt(mean + epsilon) * gains


def layer_kernel(
    per_group,
    capacity,
    decay_rate,
    tokens_hbm,
    history_length_hbm,
    inverse_hbm,
    norm_gain_hbm,
    head_gain_hbm,
    moe_gain_hbm,
    expert_group_hbm,
    expert_inner_hbm,
    route_weights_hbm,
    query_hbm,
    key_hbm,
    value_hbm,
    gate_hbm,
    out_hbm,
    state_hbm,
    expert_gate_hbm,
    expert_up_hbm,
    expert_down_hbm,
    out,
    state,
    query_w,
    key_w,
    value_w,
    gate_w,
    out_w,
    expert_gate_w,
    expert_up_w,
    expert_down_w,
    tokens,
    history_length,
    inverse,
    norm_gain,
    head_gain,
    moe_gain,
    expert_group,
    expert_inner,
    route_weights,
    key_columns,
    query_heads,
    value_heads,
    reading,
    overlap,
    meta_send,
    meta_recv,
    zsend,
    zrecv,
    hsend,
    hrecv,
    dsend,
    drecv,
    esend,
    erecv,
    osend,
    orecv,
    csend,
    crecv,
    small_sem,
    weight_sem,
    in_sem,
    load_sem,
    meta_sems,
    z_sems,
    h_sems,
    d_sems,
    e_sems,
    o_sems,
    c_sems,
):
    device = lax.axis_index("ep")
    group = device // per_group
    inner = device % per_group
    seq_count, width = tokens.shape
    group_rows = zsend.shape[1]
    slots = GROUPS * group_rows
    rows = per_group * capacity
    tiles = per_group * BLOCK
    parts = capacity * QUARTERS // BLOCK
    heads, head_width = state.shape[1], state.shape[-1]
    half = head_width // 2
    blocks = seq_count // BLOCK

    def column_peer(step):
        other = {1: group + 1 - 2 * (group % 2), 2: (group + 2) % GROUPS, 3: GROUPS - 1 - group}[step]
        return other, other * per_group + inner

    def plane_peer(step):
        other = lax.rem(inner + step, per_group)
        return other, group * per_group + other

    def remote(source, target, send_sem, recv_sem, peer):
        return pltpu.make_async_remote_copy(
            src_ref=source,
            dst_ref=target,
            send_sem=send_sem,
            recv_sem=recv_sem,
            device_id=(peer,),
            device_id_type=MESH,
        )

    def column_copy(source, target, sems, step):
        other, peer = column_peer(step)
        return remote(source.at[other], target.at[step], sems.at[0, step], sems.at[1, step], peer)

    def send_home(step):
        return remote(
            csend.at[step],
            crecv.at[group],
            c_sems.at[0, step],
            c_sems.at[1, step],
            column_peer(step)[1],
        )

    def plane_copy(source, target, sems, stage, step):
        other, peer = plane_peer(step)
        return remote(
            source.at[stage, other],
            target.at[stage, inner],
            sems.at[0, stage],
            sems.at[1, stage],
            peer,
        )

    def plane_total(source, target, sems, stage):
        others = pl.ds(0, per_group - 1)
        return remote(
            source.at[stage, others],
            target.at[stage, others],
            sems.at[0, stage],
            sems.at[1, stage],
            plane_peer(1)[1],
        )

    def each_column(act):
        for step in ORDER:
            act(step)

    def each_plane(act):
        def body(step, carry):
            act(step)
            return carry

        lax.fori_loop(1, per_group, body, 0)

    def load_all(pairs, sem):
        return [
            pltpu.make_async_copy(source, target, sem.at[index])
            for index, (source, target) in enumerate(pairs)
        ]

    barrier = pltpu.get_barrier_semaphore()

    def greet_column(step):
        pl.semaphore_signal(barrier, inc=1, device_id=(column_peer(step)[1],), device_id_type=MESH)

    def greet_plane(step):
        pl.semaphore_signal(barrier, inc=1, device_id=(plane_peer(step)[1],), device_id_type=MESH)

    smalls = load_all(
        (
            (expert_group_hbm, expert_group),
            (tokens_hbm, tokens),
            (expert_inner_hbm, expert_inner),
            (route_weights_hbm, route_weights),
            (norm_gain_hbm, norm_gain),
            (history_length_hbm, history_length),
            (inverse_hbm, inverse),
            (head_gain_hbm, head_gain),
            (moe_gain_hbm, moe_gain),
        ),
        small_sem,
    )
    weight_copies = load_all(
        (
            (query_hbm, query_w),
            (key_hbm, key_w),
            (value_hbm, value_w),
            (gate_hbm, gate_w),
            (out_hbm, out_w),
        ),
        weight_sem,
    )
    loads = load_all(
        (
            (expert_gate_hbm, expert_gate_w),
            (expert_up_hbm, expert_up_w),
            (expert_down_hbm, expert_down_w),
        ),
        load_sem,
    )

    def state_in(block):
        span = pl.ds(block * BLOCK, BLOCK)
        return pltpu.make_async_copy(state_hbm.at[span], state.at[span], in_sem.at[block])

    for copy in smalls + weight_copies[:1]:
        copy.start()
    each_column(greet_column)
    each_plane(greet_plane)
    for copy in weight_copies[1:3]:
        copy.start()

    square = (seq_count, seq_count)
    above = lax.broadcasted_iota(jnp.int32, square, 0)
    across = lax.broadcasted_iota(jnp.int32, square, 1)

    def column(row):
        return jnp.sum(jnp.where(above == across, row, 0.0), axis=1, keepdims=True)

    def earlier(columns, row):
        matched = sum((values == row).astype(jnp.float32) for values in columns)
        return jnp.sum(jnp.where(above < across, matched, 0.0), axis=0, keepdims=True)

    smalls[0].wait()
    group_row = expert_group[...].astype(jnp.float32)
    group_slot = group_row * group_rows + earlier([column(group_row)], group_row)
    slot_above = lax.broadcasted_iota(jnp.int32, (slots, seq_count), 0).astype(jnp.float32)
    placing = (slot_above == group_slot).astype(jnp.float32).astype(jnp.bfloat16)
    smalls[1].wait()
    zsend[...] = dot(placing, tokens[...]).astype(jnp.bfloat16).reshape(zsend.shape)
    with jax.named_scope("barrier"):
        pl.semaphore_wait(barrier, GROUPS - 1 + per_group - 1)
    for stage in (1, 2):
        column_copy(zsend, zrecv, z_sems, stage).start()
    for small in smalls[2:4]:
        small.wait()
    inner_rows = [expert_inner[choice : choice + 1, :].astype(jnp.float32) for choice in (0, 1)]
    expert_rows = [group_row * per_group + row for row in inner_rows]
    expert_columns = [column(row) for row in expert_rows]
    lanes = []
    for choice in (0, 1):
        slot = earlier(expert_columns, expert_rows[choice])
        lanes.append(column(inner_rows[choice] * capacity + slot + 1.0))
    for choice in (0, 1):
        weight = column(route_weights[choice : choice + 1, :])
        high = weight.astype(jnp.bfloat16).astype(jnp.float32)
        lanes += [high, weight - high]
    lane = lax.broadcasted_iota(jnp.int32, (seq_count, meta_send.shape[-1]), 1)
    token_meta = jnp.zeros(lane.shape, jnp.float32)
    for index, value in enumerate(lanes):
        token_meta = jnp.where(lane == index, value, token_meta)
    meta = dot(placing, token_meta.astype(jnp.bfloat16)).astype(jnp.bfloat16)
    meta_send[...] = meta.reshape(meta_send.shape)
    each_column(lambda step: column_copy(meta_send, meta_recv, meta_sems, step).start())
    meta_recv[0] = meta_send[group]
    zrecv[0] = zsend[group]

    def packed_places(shape, axis):
        index = lax.broadcasted_iota(jnp.int32, shape, axis)
        part = sum((index >= tiles * bound).astype(jnp.int32) for bound in range(1, parts))
        index = index - part * tiles
        place = (index & (BLOCK - 1)) * parts + part
        return (index >> 3) * capacity + (place >> 2), place & (QUARTERS - 1)

    packed_rows, packed_quarter = packed_places((1, parts * tiles), 1)
    row_names = packed_rows.astype(jnp.float32) + 1.0
    in_quarter = [(packed_quarter == part).astype(jnp.float32) for part in range(QUARTERS)]
    row_number = lax.broadcasted_iota(jnp.int32, (rows, parts * tiles), 0)
    same_row = (row_number == packed_rows).astype(jnp.float32)
    packing = jnp.concatenate([same_row * part for part in in_quarter], axis=0).astype(jnp.bfloat16)
    picks_of = {}
    weights_of = {}

    def stacked(block):
        share = block.shape[-1] // QUARTERS
        return jnp.concatenate(
            [block[:, part * share : (part + 1) * share] for part in range(QUARTERS)], axis=0
        )

    def unstacked(block):
        share = block.shape[0] // QUARTERS
        return jnp.concatenate(
            [block[part * share : (part + 1) * share] for part in range(QUARTERS)], axis=1
        )

    def take(picks, block):
        return lax.dot_general(
            picks, block, (((0,), (0,)), ((), ())), preferred_element_type=jnp.float32
        ).astype(jnp.bfloat16)

    def store_packed(sent, stage, block):
        share = block.shape[-1]
        for part in range(parts):
            sent[stage, :, :, part * share : (part + 1) * share] = block[
                part * tiles : (part + 1) * tiles
            ].reshape(per_group, BLOCK, share)

    def load_packed(landed, stage):
        block = landed[stage].reshape(tiles, landed.shape[-1])
        share = block.shape[-1] // parts
        return jnp.concatenate(
            [block[:, part * share : (part + 1) * share] for part in range(parts)], axis=0
        )

    def route(stage):
        if stage:
            column_copy(meta_send, meta_recv, meta_sems, stage).wait_recv()
        meta = meta_recv[stage].astype(jnp.float32)
        first = (row_names == meta[:, 0:1]).astype(jnp.float32)
        second = (row_names == meta[:, 1:2]).astype(jnp.float32)
        weights = first * (meta[:, 2:3] + meta[:, 3:4]) + second * (meta[:, 4:5] + meta[:, 5:6])
        both = first + second
        picks = jnp.concatenate([both * part for part in in_quarter], axis=0)
        weights = jnp.concatenate([weights * part for part in in_quarter], axis=0)
        high = weights.astype(jnp.bfloat16)
        picks_of[stage] = picks.astype(jnp.bfloat16)
        weights_of[stage] = (high, (weights - high.astype(jnp.float32)).astype(jnp.bfloat16))

    def spread(stage, received, sent, landed, sems):
        block = stacked(received[stage].astype(jnp.float32)).astype(jnp.bfloat16)
        store_packed(sent, stage, take(picks_of[stage], block))
        each_plane(lambda step: plane_copy(sent, landed, sems, stage, step).start())
        landed[stage, inner] = sent[stage, inner]

    def spread_tokens(stage):
        route(stage)
        if stage:
            column_copy(zsend, zrecv, z_sems, stage).wait_recv()
        spread(stage, zrecv, dsend, drecv, d_sems)

    def spread_heads(stage):
        if stage:
            column_copy(hsend, hrecv, h_sems, stage).wait_recv()
        spread(stage, hrecv, esend, erecv, e_sems)

    for small in smalls[4:]:
        small.wait()
    inputs = tokens[...].astype(jnp.float32)
    normed = rms(inputs, norm_gain[...]).astype(jnp.bfloat16)
    places = column(history_length[...].astype(jnp.float32))
    angles = places * inverse[...]
    cosine, sine = jnp.cos(angles), jnp.sin(angles)
    cosines = jnp.concatenate([cosine] * (2 * heads), axis=1)
    sines = jnp.concatenate([-sine, sine] * heads, axis=1)
    head_lane = lax.broadcasted_iota(jnp.int32, cosines.shape, 1)
    leading = lax.rem(head_lane, head_width) < half

    def rounded(weights):
        return dot(normed, weights[...]).astype(jnp.bfloat16).astype(jnp.float32)

    def rotated(values):
        partner = jnp.where(
            leading, jnp.roll(values, -half, axis=1), jnp.roll(values, half, axis=1)
        )
        return values * cosines + partner * sines

    def head_lanes(head):
        return slice(head * head_width, (head + 1) * head_width)

    with jax.named_scope("wait_q"):
        weight_copies[0].wait()
    queries = rotated(rounded(query_w))
    for head in range(heads):
        query_heads[head] = queries[:, head_lanes(head)]
    for block in range(blocks):
        if block == blocks - 2:
            weight_copies[3].start()
        state_in(block).start()
    with jax.named_scope("wait_k"):
        weight_copies[1].wait()
    keys = rotated(rounded(key_w)) * head_width ** (-0.5)
    with jax.named_scope("wait_v"):
        weight_copies[2].wait()
    values = rounded(value_w)
    products = keys * queries
    for head in range(heads):
        value_heads[head] = values[:, head_lanes(head)]
        overlap[head] = jnp.sum(products[:, head_lanes(head)], axis=1, keepdims=True)
    retain = [
        jnp.exp(jnp.full((1, head_width), -decay_rate[head], jnp.float32)) for head in range(heads)
    ]
    wide = (BLOCK, BLOCK * head_width)
    own = lax.broadcasted_iota(jnp.int32, wide, 0) == (
        lax.broadcasted_iota(jnp.int32, wide, 1) // head_width
    )

    def read(block, carry):
        state_in(block).wait()
        span = pl.ds(block * BLOCK, BLOCK)
        for head in range(heads):
            block_queries = query_heads[head, span, :]
            spread_queries = jnp.where(own, jnp.concatenate([block_queries] * BLOCK, axis=1), 0.0)
            high = spread_queries.astype(jnp.bfloat16).astype(jnp.float32)
            both = jnp.concatenate([high, spread_queries - high], axis=0).astype(jnp.bfloat16)
            old = state[span, head].reshape(BLOCK * head_width, head_width).astype(jnp.bfloat16)
            found = dot(both, old)
            reading[head, span, :] = (
                retain[head] * (found[:BLOCK] + found[BLOCK:])
                + overlap[head, span, :] * value_heads[head, span, :]
            )
        return carry

    def update(block, carry):
        span = pl.ds(block * BLOCK, BLOCK)
        for head in range(heads):
            lanes = slice(head * head_width, (head + 1) * head_width)
            block_values = value_heads[head, span, :]
            block_keys = key_columns[block, lanes, :]
            for index in range(BLOCK):
                sequence = block * BLOCK + index
                state[sequence, head] = (
                    retain[head] * state[sequence, head]
                    + block_keys[:, index : index + 1] * block_values[index : index + 1, :]
                )
        return carry

    def advance(first, last):
        with jax.named_scope(f"advance_{first}"):
            lax.fori_loop(first, last, update, 0)

    with jax.named_scope("spread_tokens_0"):
        spread_tokens(0)
    column_copy(zsend, zrecv, z_sems, 3).start()
    with jax.named_scope("read_a"):
        lax.fori_loop(0, blocks // 2, read, 0)
    with jax.named_scope("spread_tokens_1"):
        spread_tokens(1)
    with jax.named_scope("read"):
        lax.fori_loop(blocks // 2, blocks, read, 0)
    for copy in weight_copies[4:] + loads:
        copy.start()
    with jax.named_scope("wait_g"):
        weight_copies[3].wait()
    gating = rounded(gate_w)
    read_heads = jnp.concatenate(
        [
            rms(
                reading[head],
                head_gain[:, head_lanes(head)],
            )
            for head in range(heads)
        ],
        axis=1,
    )
    mixed_heads = (read_heads * jax.nn.silu(gating)).astype(jnp.bfloat16)
    hsend[...] = dot(placing, mixed_heads).astype(jnp.bfloat16).reshape(hsend.shape)
    each_column(lambda step: column_copy(hsend, hrecv, h_sems, step).start())
    hrecv[0] = hsend[group]
    for block in range(blocks):
        key_columns[block] = keys[block * BLOCK : (block + 1) * BLOCK].T
    with jax.named_scope("spread_heads_0"):
        spread_heads(0)
    advance(0, blocks // 6)
    with jax.named_scope("spread_tokens_2"):
        spread_tokens(2)
    for stage in ORDER[:2]:
        with jax.named_scope(f"spread_heads_{stage}"):
            spread_heads(stage)
    with jax.named_scope("wait_oe"):
        for copy in weight_copies[4:] + loads:
            copy.wait()

    def run_expert(stage):
        plane_total(dsend, drecv, d_sems, stage).wait_recv()
        plane_total(esend, erecv, e_sems, stage).wait_recv()
        token_rows = unstacked(dot(packing, load_packed(drecv, stage)))
        head_rows = unstacked(dot(packing, load_packed(erecv, stage))).astype(jnp.bfloat16)
        block = (token_rows + dot(head_rows, out_w[...])).astype(jnp.bfloat16)
        block = rms(block.astype(jnp.float32), moe_gain[...]).astype(jnp.bfloat16)
        hidden = jax.nn.silu(dot(block, expert_gate_w[...])) * dot(block, expert_up_w[...])
        block = dot(hidden.astype(jnp.bfloat16), expert_down_w[...]).astype(jnp.bfloat16)
        store_packed(osend, stage, take(packing, stacked(block)))

    def send_back(stage):
        each_plane(lambda step: plane_copy(osend, orecv, o_sems, stage, step).start())
        orecv[stage, inner] = osend[stage, inner]

    def combine(stage):
        plane_total(osend, orecv, o_sems, stage).wait_recv()
        block = load_packed(orecv, stage)
        high, low = weights_of[stage]
        csend[stage] = unstacked(dot(high, block) + dot(low, block)).astype(jnp.bfloat16)
        if stage:
            send_home(stage).start()
        else:
            crecv[group] = csend[0]

    advance(blocks // 6, 3 * blocks // 6)
    with jax.named_scope("spread_tokens_3"):
        spread_tokens(3)
    with jax.named_scope("spread_heads_3"):
        spread_heads(3)
    with jax.named_scope("run_expert_2"):
        run_expert(2)
    send_back(2)
    with jax.named_scope("run_expert_1"):
        run_expert(1)
    with jax.named_scope("run_expert_3"):
        run_expert(3)
    send_back(3)
    with jax.named_scope("combine_2"):
        combine(2)
    send_back(1)
    with jax.named_scope("run_expert_0"):
        run_expert(0)
    send_back(0)
    with jax.named_scope("combine_3"):
        combine(3)
    advance(3 * blocks // 6, 4 * blocks // 6)
    with jax.named_scope("combine_1"):
        combine(1)
    advance(4 * blocks // 6, blocks)
    with jax.named_scope("combine_0"):
        combine(0)
    with jax.named_scope("mixed"):
        mixed = (inputs + dot(mixed_heads, out_w[...])).astype(jnp.bfloat16)
    with jax.named_scope("wait_home"):
        each_column(lambda step: send_home(step).wait_recv())
    slot_across = lax.broadcasted_iota(jnp.int32, (seq_count, slots), 1).astype(jnp.float32)
    collecting = (slot_across == column(group_slot)).astype(jnp.float32).astype(jnp.bfloat16)
    block = dot(collecting, crecv[...].reshape(slots, width))
    out[...] = (mixed.astype(jnp.float32) + block).astype(jnp.bfloat16)
    each_column(lambda step: column_copy(meta_send, meta_recv, meta_sems, step).wait_send())
    each_column(lambda step: column_copy(zsend, zrecv, z_sems, step).wait_send())
    each_column(lambda step: column_copy(hsend, hrecv, h_sems, step).wait_send())
    each_column(lambda step: send_home(step).wait_send())

    for stage in range(STAGES):
        plane_total(dsend, drecv, d_sems, stage).wait_send()
        plane_total(esend, erecv, e_sems, stage).wait_send()
        plane_total(osend, orecv, o_sems, stage).wait_send()


def finish_kernel(output, state, out, state_out, sem):
    blocks = sem.shape[0] - 1
    share = state.shape[0] // blocks
    copies = [pltpu.make_async_copy(output, out, sem.at[blocks])]
    for block in range(blocks):
        span = pl.ds(block * share, share)
        copies.append(pltpu.make_async_copy(state.at[span], state_out.at[span], sem.at[block]))
    for copy in copies:
        copy.start()
    for copy in copies:
        copy.wait()


def finish(output, new_state):
    vmem = pl.BlockSpec(memory_space=pltpu.VMEM)
    hbm = pl.BlockSpec(memory_space=pl.ANY)
    return pl.pallas_call(
        finish_kernel,
        name="finish",
        out_shape=(
            jax.ShapeDtypeStruct(output.shape, output.dtype),
            jax.ShapeDtypeStruct(new_state.shape, new_state.dtype),
        ),
        in_specs=[vmem, vmem],
        out_specs=(hbm, hbm),
        scratch_shapes=[pltpu.SemaphoreType.DMA((2 * new_state.shape[0] // BLOCK + 1,))],
        compiler_params=pltpu.CompilerParams(vmem_limit_bytes=4 * 1024 * 1024),
    )(output, new_state)


def local(
    tokens,
    history_length,
    norm_gain,
    w_query,
    w_key,
    w_value,
    w_gate,
    decay_rate,
    state,
    head_gain,
    w_out,
    moe_gain,
    route_weights,
    expert_group,
    expert_inner,
    expert_gate,
    expert_up,
    expert_down,
):
    experts = lax.axis_size("ep")
    per_group = experts // GROUPS
    heads = decay_rate.shape[0]
    seq_count, model_width = tokens.shape
    head_width = state.shape[-1]
    mixed_width = heads * head_width
    half = head_width // 2
    blocks = seq_count // BLOCK
    inverse = (10000.0 ** (-np.arange(half) / half)).astype(np.float32)
    capacity = max(2, 4 * seq_count // experts)
    group_rows = -(-min(seq_count, per_group * capacity // TOP_K) // 8) * 8
    capacity += capacity % 2
    packed = capacity * QUARTERS // BLOCK
    vmem = pl.BlockSpec(memory_space=pltpu.VMEM)
    smem = pl.BlockSpec(memory_space=pltpu.SMEM)
    hbm = pl.BlockSpec(memory_space=pl.ANY)
    dma = pltpu.SemaphoreType.DMA
    bf16, f32 = jnp.bfloat16, jnp.float32

    def column_buffer(lanes):
        return [pltpu.VMEM((GROUPS, group_rows, lanes), bf16)] * 2

    def plane_buffer(lanes):
        return [pltpu.VMEM((STAGES, per_group, BLOCK, lanes * packed // QUARTERS), bf16)] * 2

    weights = (w_query, w_key, w_value, w_gate, w_out, expert_gate[0], expert_up[0], expert_down[0])
    state_bytes = state.size // head_width * max(head_width, 128) * 4

    smalls = (
        tokens,
        history_length.reshape(1, -1),
        inverse.reshape(1, -1),
        norm_gain.reshape(1, -1),
        head_gain.reshape(1, -1),
        moe_gain.reshape(1, -1),
        expert_group.reshape(1, -1),
        expert_inner.T,
        route_weights.T,
    )

    def kernel(*refs):
        layer_kernel(per_group, capacity, *refs)

    output, new_state = pl.pallas_call(
        kernel,
        name="layer",
        out_shape=(
            pltpu.VMEM((seq_count, model_width), bf16),
            pltpu.VMEM(state.shape, f32),
        ),
        in_specs=[smem] + [hbm] * 18,
        out_specs=(vmem, vmem),
        scratch_shapes=[pltpu.VMEM(weight.shape, bf16) for weight in weights]
        + [pltpu.VMEM(small.shape, small.dtype) for small in smalls]
        + [
            pltpu.VMEM((blocks, mixed_width, BLOCK), f32),
            pltpu.VMEM((heads, seq_count, head_width), f32),
            pltpu.VMEM((heads, seq_count, head_width), f32),
            pltpu.VMEM((heads, seq_count, head_width), f32),
            pltpu.VMEM((heads, seq_count, 1), f32),
        ]
        + column_buffer(128)
        + column_buffer(model_width)
        + column_buffer(mixed_width)
        + plane_buffer(model_width)
        + plane_buffer(mixed_width)
        + plane_buffer(model_width)
        + column_buffer(model_width)
        + [
            dma((9,)),
            dma((5,)),
            dma((blocks,)),
            dma((3,)),
            dma((2, GROUPS)),
            dma((2, GROUPS)),
            dma((2, GROUPS)),
            dma((2, STAGES)),
            dma((2, STAGES)),
            dma((2, STAGES)),
            dma((2, STAGES)),
        ],
        compiler_params=pltpu.CompilerParams(
            collective_id=0,
            has_side_effects=True,
            vmem_limit_bytes=63 * 1024 * 1024 - state_bytes,
        ),
    )(
        decay_rate,
        *smalls,
        w_query,
        w_key,
        w_value,
        w_gate,
        w_out,
        state,
        expert_gate[0],
        expert_up[0],
        expert_down[0],
    )
    return finish(output, new_state)


def solution(mesh):
    return jax.shard_map(
        local,
        mesh=mesh,
        in_specs=(
            P("ep", None),
            P("ep"),
            P(),
            P(),
            P(),
            P(),
            P(),
            P(),
            P("ep", None, None, None),
            P(),
            P(),
            P(),
            P("ep", None),
            P("ep"),
            P("ep", None),
            P("ep", None, None),
            P("ep", None, None),
            P("ep", None, None),
        ),
        out_specs=(P("ep", None), P("ep", None, None, None)),
        check_vma=False,
    )
```

```python
import jax
import jax.numpy as jnp
import numpy as np
from jax import lax
from jax.experimental import pallas as pl
from jax.experimental.pallas import tpu as pltpu
from jax.sharding import PartitionSpec as P

GROUPS = 4
TOP_K = 2


epsilon = 1e-06


BLOCK = 8


MESH = pl.DeviceIdType.MESH
STAGES = GROUPS
QUARTERS = 4
HALVES = 2
ORDER = (2, 3, 1)


def dot(a, b):
    return jnp.dot(a, b, preferred_element_type=jnp.float32)


def rms(values, gains):
    mean = jnp.mean(values * values, axis=-1, keepdims=True)
    return values * lax.rsqrt(mean + epsilon) * gains


def layer_kernel(
    per_group,
    capacity,
    decay_rate,
    tokens_hbm,
    history_length_hbm,
    inverse_hbm,
    norm_gain_hbm,
    head_gain_hbm,
    moe_gain_hbm,
    expert_group_hbm,
    expert_inner_hbm,
    route_weights_hbm,
    query_hbm,
    key_hbm,
    value_hbm,
    gate_hbm,
    out_hbm,
    state_hbm,
    expert_gate_hbm,
    expert_up_hbm,
    expert_down_hbm,
    out,
    state,
    query_w,
    key_w,
    value_w,
    gate_w,
    out_w,
    expert_gate_w,
    expert_up_w,
    expert_down_w,
    tokens,
    history_length,
    inverse,
    norm_gain,
    head_gain,
    moe_gain,
    expert_group,
    expert_inner,
    route_weights,
    key_columns,
    value_heads,
    query_heads,
    reading,
    overlap,
    meta_send,
    meta_recv,
    zsend,
    zrecv,
    hsend,
    hrecv,
    dsend,
    drecv,
    esend,
    erecv,
    osend,
    orecv,
    csend,
    crecv,
    small_sem,
    weight_sem,
    in_sem,
    load_sem,
    meta_sems,
    z_sems,
    h_sems,
    d_sems,
    e_sems,
    o_sems,
    c_sems,
):
    device = lax.axis_index("ep")
    group = device // per_group
    inner = device % per_group
    seq_count, width = tokens.shape
    group_rows = zsend.shape[1]
    slots = GROUPS * group_rows
    rows = per_group * capacity
    tiles = per_group * BLOCK
    parts = capacity * QUARTERS // BLOCK
    heads, head_width = state.shape[1], state.shape[-1]
    half = head_width // 2
    blocks = seq_count // BLOCK

    def column_peer(step):
        other = {1: group + 1 - 2 * (group % 2), 2: (group + 2) % GROUPS, 3: GROUPS - 1 - group}[step]
        return other, other * per_group + inner

    def plane_peer(step):
        other = lax.rem(inner + step, per_group)
        return other, group * per_group + other

    def remote(source, target, send_sem, recv_sem, peer):
        return pltpu.make_async_remote_copy(
            src_ref=source,
            dst_ref=target,
            send_sem=send_sem,
            recv_sem=recv_sem,
            device_id=(peer,),
            device_id_type=MESH,
        )

    def column_copy(source, target, sems, step):
        other, peer = column_peer(step)
        return remote(source.at[other], target.at[step], sems.at[0], sems.at[step], peer)

    def column_sent(source, target, sems):
        others = pl.ds(1, GROUPS - 1)
        return remote(source.at[others], target.at[others], sems.at[0], sems.at[1], column_peer(1)[1])

    def send_home(step, half):
        index = step * HALVES + half
        return remote(
            csend.at[step, half],
            crecv.at[group, half],
            c_sems.at[0],
            c_sems.at[index],
            column_peer(step)[1],
        )

    def plane_copy(source, target, sems, stage, step):
        other, peer = plane_peer(step)
        return remote(
            source.at[stage, other],
            target.at[stage, inner],
            sems.at[0],
            sems.at[stage + 1],
            peer,
        )

    def plane_total(source, target, sems, stage):
        others = pl.ds(0, per_group - 1)
        return remote(
            source.at[stage, others],
            target.at[stage, others],
            sems.at[0],
            sems.at[stage + 1],
            plane_peer(1)[1],
        )

    def plane_sent(source, target, sems):
        others = pl.ds(0, per_group - 1)
        return remote(
            source.at[:, others], target.at[:, others], sems.at[0], sems.at[1], plane_peer(1)[1]
        )

    def each_column(act):
        for step in ORDER:
            act(step)

    def each_plane(act):
        def body(step, carry):
            act(step)
            return carry

        lax.fori_loop(1, per_group, body, 0)

    def load_all(pairs, sem):
        return [
            pltpu.make_async_copy(source, target, sem.at[index])
            for index, (source, target) in enumerate(pairs)
        ]

    barrier = pltpu.get_barrier_semaphore()

    def greet_column(step):
        pl.semaphore_signal(barrier, inc=1, device_id=(column_peer(step)[1],), device_id_type=MESH)

    def greet_plane(step):
        pl.semaphore_signal(barrier, inc=1, device_id=(plane_peer(step)[1],), device_id_type=MESH)

    smalls = load_all(
        (
            (expert_group_hbm, expert_group),
            (tokens_hbm, tokens),
            (expert_inner_hbm, expert_inner),
            (route_weights_hbm, route_weights),
            (norm_gain_hbm, norm_gain),
            (history_length_hbm, history_length),
            (inverse_hbm, inverse),
            (head_gain_hbm, head_gain),
            (moe_gain_hbm, moe_gain),
        ),
        small_sem,
    )
    weight_copies = load_all(
        (
            (query_hbm, query_w),
            (key_hbm, key_w),
            (value_hbm, value_w),
            (gate_hbm, gate_w),
            (out_hbm, out_w),
        ),
        weight_sem,
    )
    loads = load_all(
        (
            (expert_gate_hbm, expert_gate_w),
            (expert_up_hbm, expert_up_w),
            (expert_down_hbm, expert_down_w),
        ),
        load_sem,
    )

    def state_in(block):
        span = pl.ds(block * BLOCK, BLOCK)
        return pltpu.make_async_copy(state_hbm.at[span], state.at[span], in_sem.at[block])

    for copy in smalls + weight_copies[:1]:
        copy.start()
    each_column(greet_column)
    each_plane(greet_plane)
    for copy in weight_copies[1:3]:
        copy.start()

    square = (seq_count, seq_count)
    above = lax.broadcasted_iota(jnp.int32, square, 0)
    across = lax.broadcasted_iota(jnp.int32, square, 1)

    def column(row):
        return jnp.sum(jnp.where(above == across, row, 0.0), axis=1, keepdims=True)

    def earlier(columns, row):
        matched = sum((values == row).astype(jnp.float32) for values in columns)
        return jnp.sum(jnp.where(above < across, matched, 0.0), axis=0, keepdims=True)

    smalls[0].wait()
    group_row = expert_group[...].astype(jnp.float32)
    group_slot = group_row * group_rows + earlier([column(group_row)], group_row)
    slot_above = lax.broadcasted_iota(jnp.int32, (slots, seq_count), 0).astype(jnp.float32)
    placing = (slot_above == group_slot).astype(jnp.float32).astype(jnp.bfloat16)
    smalls[1].wait()
    zsend[...] = dot(placing, tokens[...]).astype(jnp.bfloat16).reshape(zsend.shape)
    with jax.named_scope("barrier"):
        pl.semaphore_wait(barrier, GROUPS - 1 + per_group - 1)
    outer = group * (GROUPS - 1 - group) == 0

    def send_tokens(stage, held):
        @pl.when(outer if held else jnp.logical_not(outer))
        def start():
            column_copy(zsend, zrecv, z_sems, stage).start()

    send_tokens(2, True)
    send_tokens(1, False)
    for block in range(2):
        state_in(block).start()
    for small in smalls[2:4]:
        small.wait()
    inner_rows = [expert_inner[choice : choice + 1, :].astype(jnp.float32) for choice in (0, 1)]
    expert_rows = [group_row * per_group + row for row in inner_rows]
    expert_columns = [column(row) for row in expert_rows]
    lanes = []
    for choice in (0, 1):
        slot = earlier(expert_columns, expert_rows[choice])
        lanes.append(column(inner_rows[choice] * capacity + slot + 1.0))
    for choice in (0, 1):
        weight = column(route_weights[choice : choice + 1, :])
        high = weight.astype(jnp.bfloat16).astype(jnp.float32)
        lanes += [high, weight - high]
    lane = lax.broadcasted_iota(jnp.int32, (seq_count, meta_send.shape[-1]), 1)
    token_meta = jnp.zeros(lane.shape, jnp.float32)
    for index, value in enumerate(lanes):
        token_meta = jnp.where(lane == index, value, token_meta)
    meta = dot(placing, token_meta.astype(jnp.bfloat16)).astype(jnp.bfloat16)
    meta_send[...] = meta.reshape(meta_send.shape)
    each_column(lambda step: column_copy(meta_send, meta_recv, meta_sems, step).start())
    meta_recv[0] = meta_send[group]
    zrecv[0] = zsend[group]

    def packed_places(shape, axis):
        index = lax.broadcasted_iota(jnp.int32, shape, axis)
        part = sum((index >= tiles * bound).astype(jnp.int32) for bound in range(1, parts))
        index = index - part * tiles
        place = (index & (BLOCK - 1)) * parts + part
        return (index >> 3) * capacity + (place >> 2), place & (QUARTERS - 1)

    packed_rows, packed_quarter = packed_places((1, parts * tiles), 1)
    row_names = packed_rows.astype(jnp.float32) + 1.0
    in_quarter = [(packed_quarter == part).astype(jnp.float32) for part in range(QUARTERS)]
    row_number = lax.broadcasted_iota(jnp.int32, (rows, parts * tiles), 0)
    same_row = (row_number == packed_rows).astype(jnp.float32)
    packing = jnp.concatenate([same_row * part for part in in_quarter], axis=0).astype(jnp.bfloat16)
    picks_of = {}
    weights_of = {}

    def stacked(block):
        share = block.shape[-1] // QUARTERS
        return jnp.concatenate(
            [block[:, part * share : (part + 1) * share] for part in range(QUARTERS)], axis=0
        )

    def unstacked(block):
        share = block.shape[0] // QUARTERS
        return jnp.concatenate(
            [block[part * share : (part + 1) * share] for part in range(QUARTERS)], axis=1
        )

    def take(picks, block):
        return lax.dot_general(
            picks, block, (((0,), (0,)), ((), ())), preferred_element_type=jnp.float32
        ).astype(jnp.bfloat16)

    def store_packed(sent, stage, block):
        share = block.shape[-1]
        for part in range(parts):
            sent[stage, :, :, part * share : (part + 1) * share] = block[
                part * tiles : (part + 1) * tiles
            ].reshape(per_group, BLOCK, share)

    def load_packed(landed, stage):
        block = landed[stage].reshape(tiles, landed.shape[-1])
        share = block.shape[-1] // parts
        return jnp.concatenate(
            [block[:, part * share : (part + 1) * share] for part in range(parts)], axis=0
        )

    def route(stage):
        if stage:
            column_copy(meta_send, meta_recv, meta_sems, stage).wait_recv()
        meta = meta_recv[stage].astype(jnp.float32)
        first = (row_names == meta[:, 0:1]).astype(jnp.float32)
        second = (row_names == meta[:, 1:2]).astype(jnp.float32)
        weights = first * (meta[:, 2:3] + meta[:, 3:4]) + second * (meta[:, 4:5] + meta[:, 5:6])
        both = first + second
        picks = jnp.concatenate([both * part for part in in_quarter], axis=0)
        weights = jnp.concatenate([weights * part for part in in_quarter], axis=0)
        high = weights.astype(jnp.bfloat16)
        picks_of[stage] = picks.astype(jnp.bfloat16)
        weights_of[stage] = (high, (weights - high.astype(jnp.float32)).astype(jnp.bfloat16))

    def spread(stage, picks, received, sent, landed, sems):
        block = stacked(received[stage].astype(jnp.float32)).astype(jnp.bfloat16)
        store_packed(sent, stage, take(picks, block))
        each_plane(lambda step: plane_copy(sent, landed, sems, stage, step).start())
        landed[stage, inner] = sent[stage, inner]

    def spread_tokens(stage):
        route(stage)
        if stage:
            column_copy(zsend, zrecv, z_sems, stage).wait_recv()
        spread(stage, picks_of[stage], zrecv, dsend, drecv, d_sems)

    def spread_nearer(first):
        stage = jnp.where(outer == first, 1, 2)
        near, far = (picks_of[1], picks_of[2]) if first else (picks_of[2], picks_of[1])
        picks = jnp.where(outer, near.astype(jnp.float32), far.astype(jnp.float32))
        remote(
            zsend.at[0],
            zrecv.at[stage],
            z_sems.at[0],
            z_sems.at[stage],
            plane_peer(1)[1],
        ).wait_recv()
        spread(stage, picks.astype(jnp.bfloat16), zrecv, dsend, drecv, d_sems)

    def spread_heads(stage):
        if stage:
            column_copy(hsend, hrecv, h_sems, stage).wait_recv()
        spread(stage, picks_of[stage], hrecv, esend, erecv, e_sems)

    for small in smalls[4:]:
        small.wait()
    inputs = tokens[...].astype(jnp.float32)
    normed = rms(inputs, norm_gain[...]).astype(jnp.bfloat16)
    places = column(history_length[...].astype(jnp.float32))
    angles = places * inverse[...]
    cosine, sine = jnp.cos(angles), jnp.sin(angles)
    cosines = jnp.concatenate([cosine] * (2 * heads), axis=1)
    sines = jnp.concatenate([-sine, sine] * heads, axis=1)
    head_lane = lax.broadcasted_iota(jnp.int32, cosines.shape, 1)
    leading = lax.rem(head_lane, head_width) < half

    def rounded(weights):
        return dot(normed, weights[...]).astype(jnp.bfloat16).astype(jnp.float32)

    def rotated(values):
        partner = jnp.where(
            leading, jnp.roll(values, -half, axis=1), jnp.roll(values, half, axis=1)
        )
        return values * cosines + partner * sines

    def head_lanes(head):
        return slice(head * head_width, (head + 1) * head_width)

    with jax.named_scope("wait_q"):
        weight_copies[0].wait()
    queries = rotated(rounded(query_w))
    for head in range(heads):
        query_heads[head] = queries[:, head_lanes(head)]
    send_tokens(1, True)
    send_tokens(2, False)
    for block in range(2, blocks):
        if block == blocks - 2:
            weight_copies[3].start()
        state_in(block).start()
    with jax.named_scope("wait_k"):
        weight_copies[1].wait()
    keys = rotated(rounded(key_w)) * head_width ** (-0.5)
    with jax.named_scope("wait_v"):
        weight_copies[2].wait()
    values = rounded(value_w)
    products = keys * queries
    for head in range(heads):
        value_heads[head] = values[:, head_lanes(head)]
        overlap[head] = jnp.sum(products[:, head_lanes(head)], axis=1, keepdims=True)
    retain = [
        jnp.exp(jnp.full((1, head_width), -decay_rate[head], jnp.float32)) for head in range(heads)
    ]
    wide = (BLOCK, BLOCK * head_width)
    own = lax.broadcasted_iota(jnp.int32, wide, 0) == (
        lax.broadcasted_iota(jnp.int32, wide, 1) // head_width
    )

    def read(block, carry):
        state_in(block).wait()
        span = pl.ds(block * BLOCK, BLOCK)
        for head in range(heads):
            block_queries = query_heads[head, span, :]
            spread_queries = jnp.where(own, jnp.concatenate([block_queries] * BLOCK, axis=1), 0.0)
            high = spread_queries.astype(jnp.bfloat16).astype(jnp.float32)
            both = jnp.concatenate([high, spread_queries - high], axis=0).astype(jnp.bfloat16)
            old = state[span, head].reshape(BLOCK * head_width, head_width).astype(jnp.bfloat16)
            found = dot(both, old)
            reading[head, span, :] = (
                retain[head] * (found[:BLOCK] + found[BLOCK:])
                + overlap[head, span, :] * value_heads[head, span, :]
            )
        return carry

    def update(block, carry):
        span = pl.ds(block * BLOCK, BLOCK)
        for head in range(heads):
            lanes = slice(head * head_width, (head + 1) * head_width)
            block_values = value_heads[head, span, :]
            block_keys = key_columns[block, lanes, :]
            for index in range(BLOCK):
                sequence = block * BLOCK + index
                state[sequence, head] = (
                    retain[head] * state[sequence, head]
                    + block_keys[:, index : index + 1] * block_values[index : index + 1, :]
                )
        return carry

    def advance(first, last):
        with jax.named_scope(f"advance_{first}"):
            lax.fori_loop(first, last, update, 0)

    with jax.named_scope("spread_tokens_0"):
        spread_tokens(0)
    with jax.named_scope("read_a"):
        lax.fori_loop(0, blocks // 2, read, 0)
    send_tokens(3, True)
    with jax.named_scope("spread_near"):
        for stage in (1, 2):
            route(stage)
        spread_nearer(True)
    with jax.named_scope("read"):
        lax.fori_loop(blocks // 2, blocks, read, 0)
    for copy in weight_copies[4:] + loads:
        copy.start()
    with jax.named_scope("wait_g"):
        weight_copies[3].wait()
    gating = rounded(gate_w)
    read_heads = jnp.concatenate(
        [
            rms(
                reading[head],
                head_gain[:, head_lanes(head)],
            )
            for head in range(heads)
        ],
        axis=1,
    )
    mixed_heads = (read_heads * jax.nn.silu(gating)).astype(jnp.bfloat16)
    hsend[...] = dot(placing, mixed_heads).astype(jnp.bfloat16).reshape(hsend.shape)
    each_column(lambda step: column_copy(hsend, hrecv, h_sems, step).start())
    hrecv[0] = hsend[group]
    half_width = width // HALVES

    def run_expert(stage, send):
        plane_total(dsend, drecv, d_sems, stage).wait_recv()
        token_rows = unstacked(dot(packing, load_packed(drecv, stage)))
        plane_total(esend, erecv, e_sems, stage).wait_recv()
        head_rows = unstacked(dot(packing, load_packed(erecv, stage))).astype(jnp.bfloat16)
        block = (token_rows + dot(head_rows, out_w[...])).astype(jnp.bfloat16)
        block = rms(block.astype(jnp.float32), moe_gain[...]).astype(jnp.bfloat16)
        hidden = jax.nn.silu(dot(block, expert_gate_w[...])) * dot(block, expert_up_w[...])
        hidden = hidden.astype(jnp.bfloat16)
        for half in range(HALVES):
            lanes = slice(half * half_width, (half + 1) * half_width)
            block = dot(hidden, expert_down_w[:, lanes]).astype(jnp.bfloat16)
            store_packed(osend, stage * HALVES + half, take(packing, stacked(block)))
            if send:
                send_back(stage, half)

    def send_back(stage, half):
        index = stage * HALVES + half
        each_plane(lambda step: plane_copy(osend, orecv, o_sems, index, step).start())
        orecv[index, inner] = osend[index, inner]

    def combine(stage, half):
        index = stage * HALVES + half
        plane_total(osend, orecv, o_sems, index).wait_recv()
        block = load_packed(orecv, index)
        high, low = weights_of[stage]
        block = unstacked(dot(high, block) + dot(low, block)).astype(jnp.bfloat16)
        if stage:
            csend[stage, half] = block
            send_home(stage, half).start()
        else:
            crecv[group, half] = block

    def combine_all(stage):
        for half in range(HALVES):
            with jax.named_scope(f"combine_{stage}_{half}"):
                combine(stage, half)

    with jax.named_scope("spread_heads_0"):
        spread_heads(0)
    with jax.named_scope("spread_far"):
        spread_nearer(False)
    send_tokens(3, False)
    for block in range(blocks):
        key_columns[block] = keys[block * BLOCK : (block + 1) * BLOCK].T
    for stage in (2, 1):
        with jax.named_scope(f"spread_heads_{stage}"):
            spread_heads(stage)
    with jax.named_scope("spread_tokens_3"):
        spread_tokens(3)
    with jax.named_scope("spread_heads_3"):
        spread_heads(3)
    with jax.named_scope("wait_oe"):
        for copy in weight_copies[4:] + loads:
            copy.wait()

    with jax.named_scope("run_expert_0"):
        run_expert(0, False)
    for stage in (2, 3):
        with jax.named_scope(f"run_expert_{stage}"):
            run_expert(stage, True)
    combine_all(2)
    with jax.named_scope("run_expert_1"):
        run_expert(1, True)
    combine_all(3)
    for half in range(HALVES):
        send_back(0, half)
    with jax.named_scope("mixed"):
        mixed = (inputs + dot(mixed_heads, out_w[...])).astype(jnp.bfloat16)
    advance(0, 2 * blocks // 3)
    combine_all(1)
    combine_all(0)
    advance(2 * blocks // 3, blocks)
    slot_across = lax.broadcasted_iota(jnp.int32, (seq_count, slots), 1).astype(jnp.float32)
    collecting = (slot_across == column(group_slot)).astype(jnp.float32).astype(jnp.bfloat16)
    for half in range(HALVES):
        lanes = slice(half * half_width, (half + 1) * half_width)
        with jax.named_scope(f"wait_home_{half}"):
            each_column(lambda step: send_home(step, half).wait_recv())
        block = dot(collecting, crecv[:, half].reshape(slots, half_width))
        out[:, lanes] = (mixed[:, lanes].astype(jnp.float32) + block).astype(jnp.bfloat16)
    column_sent(meta_send, meta_recv, meta_sems).wait_send()
    column_sent(zsend, zrecv, z_sems).wait_send()
    column_sent(hsend, hrecv, h_sems).wait_send()
    column_sent(csend, crecv, c_sems).wait_send()
    plane_sent(dsend, drecv, d_sems).wait_send()
    plane_sent(esend, erecv, e_sems).wait_send()
    plane_sent(osend, orecv, o_sems).wait_send()


def finish_kernel(output, state, out, state_out, sem):
    blocks = sem.shape[0] - 1
    share = state.shape[0] // blocks
    copies = [pltpu.make_async_copy(output, out, sem.at[blocks])]
    for block in range(blocks):
        span = pl.ds(block * share, share)
        copies.append(pltpu.make_async_copy(state.at[span], state_out.at[span], sem.at[block]))
    for copy in copies:
        copy.start()
    for copy in copies:
        copy.wait()


def finish(output, new_state):
    vmem = pl.BlockSpec(memory_space=pltpu.VMEM)
    hbm = pl.BlockSpec(memory_space=pl.ANY)
    return pl.pallas_call(
        finish_kernel,
        name="finish",
        out_shape=(
            jax.ShapeDtypeStruct(output.shape, output.dtype),
            jax.ShapeDtypeStruct(new_state.shape, new_state.dtype),
        ),
        in_specs=[vmem, vmem],
        out_specs=(hbm, hbm),
        scratch_shapes=[pltpu.SemaphoreType.DMA((2 * new_state.shape[0] // BLOCK + 1,))],
        compiler_params=pltpu.CompilerParams(vmem_limit_bytes=4 * 1024 * 1024),
    )(output, new_state)


def local(
    tokens,
    history_length,
    norm_gain,
    w_query,
    w_key,
    w_value,
    w_gate,
    decay_rate,
    state,
    head_gain,
    w_out,
    moe_gain,
    route_weights,
    expert_group,
    expert_inner,
    expert_gate,
    expert_up,
    expert_down,
):
    experts = lax.axis_size("ep")
    per_group = experts // GROUPS
    heads = decay_rate.shape[0]
    seq_count, model_width = tokens.shape
    head_width = state.shape[-1]
    mixed_width = heads * head_width
    half = head_width // 2
    blocks = seq_count // BLOCK
    inverse = (10000.0 ** (-np.arange(half) / half)).astype(np.float32)
    capacity = max(2, 4 * seq_count // experts)
    group_rows = -(-min(seq_count, per_group * capacity // TOP_K) // 8) * 8
    capacity += capacity % 2
    packed = capacity * QUARTERS // BLOCK
    half_lanes = model_width // HALVES * packed // QUARTERS
    vmem = pl.BlockSpec(memory_space=pltpu.VMEM)
    smem = pl.BlockSpec(memory_space=pltpu.SMEM)
    hbm = pl.BlockSpec(memory_space=pl.ANY)
    dma = pltpu.SemaphoreType.DMA
    bf16, f32 = jnp.bfloat16, jnp.float32

    def column_buffer(lanes):
        return [pltpu.VMEM((GROUPS, group_rows, lanes), bf16)] * 2

    def plane_buffer(lanes):
        return [pltpu.VMEM((STAGES, per_group, BLOCK, lanes * packed // QUARTERS), bf16)] * 2

    weights = (w_query, w_key, w_value, w_gate, w_out, expert_gate[0], expert_up[0], expert_down[0])
    state_bytes = state.size // head_width * max(head_width, 128) * 4

    smalls = (
        tokens,
        history_length.reshape(1, -1),
        inverse.reshape(1, -1),
        norm_gain.reshape(1, -1),
        head_gain.reshape(1, -1),
        moe_gain.reshape(1, -1),
        expert_group.reshape(1, -1),
        expert_inner.T,
        route_weights.T,
    )

    def kernel(*refs):
        layer_kernel(per_group, capacity, *refs)

    output, new_state = pl.pallas_call(
        kernel,
        name="layer",
        out_shape=(
            pltpu.VMEM((seq_count, model_width), bf16),
            pltpu.VMEM(state.shape, f32),
        ),
        in_specs=[smem] + [hbm] * 18,
        out_specs=(vmem, vmem),
        scratch_shapes=[pltpu.VMEM(weight.shape, bf16) for weight in weights]
        + [pltpu.VMEM(small.shape, small.dtype) for small in smalls]
        + [
            pltpu.VMEM((blocks, mixed_width, BLOCK), f32),
            pltpu.VMEM((heads, seq_count, head_width), f32),
            pltpu.VMEM((heads, seq_count, head_width), f32),
            pltpu.VMEM((heads, seq_count, head_width), f32),
            pltpu.VMEM((heads, seq_count, 1), f32),
        ]
        + column_buffer(128)
        + column_buffer(model_width)
        + column_buffer(mixed_width)
        + plane_buffer(model_width)
        + plane_buffer(mixed_width)
        + [pltpu.VMEM((STAGES * HALVES, per_group, BLOCK, half_lanes), bf16)] * 2
        + [pltpu.VMEM((GROUPS, HALVES, group_rows, model_width // HALVES), bf16)] * 2
        + [
            dma((9,)),
            dma((5,)),
            dma((blocks,)),
            dma((3,)),
            dma((GROUPS,)),
            dma((GROUPS,)),
            dma((GROUPS,)),
            dma((STAGES + 1,)),
            dma((STAGES + 1,)),
            dma((STAGES * HALVES + 1,)),
            dma((GROUPS * HALVES,)),
        ],
        compiler_params=pltpu.CompilerParams(
            collective_id=0,
            has_side_effects=True,
            vmem_limit_bytes=63 * 1024 * 1024 - state_bytes,
        ),
    )(
        decay_rate,
        *smalls,
        w_query,
        w_key,
        w_value,
        w_gate,
        w_out,
        state,
        expert_gate[0],
        expert_up[0],
        expert_down[0],
    )
    return finish(output, new_state)


def solution(mesh):
    return jax.shard_map(
        local,
        mesh=mesh,
        in_specs=(
            P("ep", None),
            P("ep"),
            P(),
            P(),
            P(),
            P(),
            P(),
            P(),
            P("ep", None, None, None),
            P(),
            P(),
            P(),
            P("ep", None),
            P("ep"),
            P("ep", None),
            P("ep", None, None),
            P("ep", None, None),
            P("ep", None, None),
        ),
        out_specs=(P("ep", None), P("ep", None, None, None)),
        check_vma=False,
    )
```

```python
import jax
import jax.numpy as jnp
import numpy as np
from jax import lax
from jax.experimental import pallas as pl
from jax.experimental.pallas import tpu as pltpu
from jax.sharding import PartitionSpec as P

GROUPS = 4
TOP_K = 2


epsilon = 1e-06


BLOCK = 8


MESH = pl.DeviceIdType.MESH
STAGES = GROUPS
QUARTERS = 4
HALVES = 2
ORDER = (2, 3, 1)


def dot(a, b):
    return jnp.dot(a, b, preferred_element_type=jnp.float32)


def rms(values, gains):
    mean = jnp.mean(values * values, axis=-1, keepdims=True)
    return values * lax.rsqrt(mean + epsilon) * gains


def layer_kernel(
    per_group,
    capacity,
    decay_rate,
    tokens_hbm,
    history_length_hbm,
    inverse_hbm,
    norm_gain_hbm,
    head_gain_hbm,
    moe_gain_hbm,
    expert_group_hbm,
    expert_inner_hbm,
    route_weights_hbm,
    query_hbm,
    key_hbm,
    value_hbm,
    gate_hbm,
    out_hbm,
    state_hbm,
    expert_gate_hbm,
    expert_up_hbm,
    expert_down_hbm,
    out,
    state,
    query_w,
    key_w,
    value_w,
    gate_w,
    out_w,
    expert_gate_w,
    expert_up_w,
    expert_down_w,
    tokens,
    history_length,
    inverse,
    norm_gain,
    head_gain,
    moe_gain,
    expert_group,
    expert_inner,
    route_weights,
    key_columns,
    value_heads,
    query_heads,
    reading,
    overlap,
    meta_send,
    meta_recv,
    zsend,
    zrecv,
    hsend,
    hrecv,
    dsend,
    drecv,
    esend,
    erecv,
    osend,
    orecv,
    csend,
    crecv,
    small_sem,
    weight_sem,
    in_sem,
    load_sem,
    meta_sems,
    z_sems,
    h_sems,
    d_sems,
    e_sems,
    o_sems,
    c_sems,
):
    device = lax.axis_index("ep")
    group = device // per_group
    inner = device % per_group
    seq_count, width = tokens.shape
    group_rows = zsend.shape[1]
    slots = GROUPS * group_rows
    rows = per_group * capacity
    tiles = per_group * BLOCK
    parts = capacity * QUARTERS // BLOCK
    heads, head_width = state.shape[1], state.shape[-1]
    half = head_width // 2
    blocks = seq_count // BLOCK

    side = group // 2
    within = group * (GROUPS - 1 - group) // 2
    others = {1: group + 1 - 2 * (group % 2), 2: 3 * (1 - side), 3: 2 - side}
    landing = {1: 1, 2: 2 + within, 3: 2 + within}

    def column_peer(step):
        return others[step], others[step] * per_group + inner

    def plane_peer(step):
        other = lax.rem(inner + step, per_group)
        return other, group * per_group + other

    def remote(source, target, send_sem, recv_sem, peer):
        return pltpu.make_async_remote_copy(
            src_ref=source,
            dst_ref=target,
            send_sem=send_sem,
            recv_sem=recv_sem,
            device_id=(peer,),
            device_id_type=MESH,
        )

    def column_copy(source, target, sems, step):
        other, peer = column_peer(step)
        place = landing[step]
        return remote(source.at[other], target.at[place], sems.at[0], sems.at[place], peer)

    def column_landed(source, target, sems, step):
        return remote(source.at[0], target.at[step], sems.at[0], sems.at[step], column_peer(1)[1])

    def column_sent(source, target, sems):
        others = pl.ds(1, GROUPS - 1)
        return remote(source.at[others], target.at[others], sems.at[0], sems.at[1], column_peer(1)[1])

    def send_home(step, half):
        return remote(
            csend.at[step, half],
            crecv.at[group, half],
            c_sems.at[0],
            c_sems.at[landing[step] * HALVES + half],
            column_peer(step)[1],
        )

    def home_landed(step, half):
        return remote(
            csend.at[step, half],
            crecv.at[step, half],
            c_sems.at[0],
            c_sems.at[step * HALVES + half],
            column_peer(step)[1],
        )

    def plane_copy(source, target, sems, stage, step):
        other, peer = plane_peer(step)
        return remote(
            source.at[stage, other],
            target.at[stage, inner],
            sems.at[0],
            sems.at[stage + 1],
            peer,
        )

    def plane_total(source, target, sems, stage):
        others = pl.ds(0, per_group - 1)
        return remote(
            source.at[stage, others],
            target.at[stage, others],
            sems.at[0],
            sems.at[stage + 1],
            plane_peer(1)[1],
        )

    def plane_sent(source, target, sems):
        others = pl.ds(0, per_group - 1)
        return remote(
            source.at[:, others], target.at[:, others], sems.at[0], sems.at[1], plane_peer(1)[1]
        )

    def each_column(act):
        for step in ORDER:
            act(step)

    def each_plane(act):
        def body(step, carry):
            act(step)
            return carry

        lax.fori_loop(1, per_group, body, 0)

    def load_all(pairs, sem):
        return [
            pltpu.make_async_copy(source, target, sem.at[index])
            for index, (source, target) in enumerate(pairs)
        ]

    barrier = pltpu.get_barrier_semaphore()

    def greet_column(step):
        pl.semaphore_signal(barrier, inc=1, device_id=(column_peer(step)[1],), device_id_type=MESH)

    def greet_plane(step):
        pl.semaphore_signal(barrier, inc=1, device_id=(plane_peer(step)[1],), device_id_type=MESH)

    smalls = load_all(
        (
            (expert_group_hbm, expert_group),
            (tokens_hbm, tokens),
            (expert_inner_hbm, expert_inner),
            (route_weights_hbm, route_weights),
            (norm_gain_hbm, norm_gain),
            (history_length_hbm, history_length),
            (inverse_hbm, inverse),
            (head_gain_hbm, head_gain),
            (moe_gain_hbm, moe_gain),
        ),
        small_sem,
    )
    weight_copies = load_all(
        (
            (query_hbm, query_w),
            (key_hbm, key_w),
            (value_hbm, value_w),
            (gate_hbm, gate_w),
            (out_hbm, out_w),
        ),
        weight_sem,
    )
    loads = load_all(
        (
            (expert_gate_hbm, expert_gate_w),
            (expert_up_hbm, expert_up_w),
            (expert_down_hbm, expert_down_w),
        ),
        load_sem,
    )

    def state_in(block):
        span = pl.ds(block * BLOCK, BLOCK)
        return pltpu.make_async_copy(state_hbm.at[span], state.at[span], in_sem.at[block])

    for copy in smalls + weight_copies[:1]:
        copy.start()
    each_column(greet_column)
    each_plane(greet_plane)
    for copy in weight_copies[1:3]:
        copy.start()

    square = (seq_count, seq_count)
    above = lax.broadcasted_iota(jnp.int32, square, 0)
    across = lax.broadcasted_iota(jnp.int32, square, 1)

    def column(row):
        return jnp.sum(jnp.where(above == across, row, 0.0), axis=1, keepdims=True)

    def earlier(columns, row):
        matched = sum((values == row).astype(jnp.float32) for values in columns)
        return jnp.sum(jnp.where(above < across, matched, 0.0), axis=0, keepdims=True)

    smalls[0].wait()
    group_row = expert_group[...].astype(jnp.float32)
    group_slot = group_row * group_rows + earlier([column(group_row)], group_row)
    slot_above = lax.broadcasted_iota(jnp.int32, (slots, seq_count), 0).astype(jnp.float32)
    placing = (slot_above == group_slot).astype(jnp.float32).astype(jnp.bfloat16)
    smalls[1].wait()
    zsend[...] = dot(placing, tokens[...]).astype(jnp.bfloat16).reshape(zsend.shape)
    with jax.named_scope("barrier"):
        pl.semaphore_wait(barrier, GROUPS - 1 + per_group - 1)
    outer = within == 0

    def send_tokens(stage, held):
        @pl.when(outer if held else jnp.logical_not(outer))
        def start():
            column_copy(zsend, zrecv, z_sems, stage).start()

    send_tokens(3, True)
    send_tokens(1, False)
    for block in range(2):
        state_in(block).start()
    for small in smalls[2:4]:
        small.wait()
    inner_rows = [expert_inner[choice : choice + 1, :].astype(jnp.float32) for choice in (0, 1)]
    expert_rows = [group_row * per_group + row for row in inner_rows]
    expert_columns = [column(row) for row in expert_rows]
    lanes = []
    for choice in (0, 1):
        slot = earlier(expert_columns, expert_rows[choice])
        lanes.append(column(inner_rows[choice] * capacity + slot + 1.0))
    for choice in (0, 1):
        weight = column(route_weights[choice : choice + 1, :])
        high = weight.astype(jnp.bfloat16).astype(jnp.float32)
        lanes += [high, weight - high]
    lane = lax.broadcasted_iota(jnp.int32, (seq_count, meta_send.shape[-1]), 1)
    token_meta = jnp.zeros(lane.shape, jnp.float32)
    for index, value in enumerate(lanes):
        token_meta = jnp.where(lane == index, value, token_meta)
    meta = dot(placing, token_meta.astype(jnp.bfloat16)).astype(jnp.bfloat16)
    meta_send[...] = meta.reshape(meta_send.shape)
    each_column(lambda step: column_copy(meta_send, meta_recv, meta_sems, step).start())
    meta_recv[0] = meta_send[group]
    zrecv[0] = zsend[group]

    def packed_places(shape, axis):
        index = lax.broadcasted_iota(jnp.int32, shape, axis)
        part = sum((index >= tiles * bound).astype(jnp.int32) for bound in range(1, parts))
        index = index - part * tiles
        place = (index & (BLOCK - 1)) * parts + part
        return (index >> 3) * capacity + (place >> 2), place & (QUARTERS - 1)

    packed_rows, packed_quarter = packed_places((1, parts * tiles), 1)
    row_names = packed_rows.astype(jnp.float32) + 1.0
    in_quarter = [(packed_quarter == part).astype(jnp.float32) for part in range(QUARTERS)]
    row_number = lax.broadcasted_iota(jnp.int32, (rows, parts * tiles), 0)
    same_row = (row_number == packed_rows).astype(jnp.float32)
    packing = jnp.concatenate([same_row * part for part in in_quarter], axis=0).astype(jnp.bfloat16)
    picks_of = {}
    weights_of = {}

    def stacked(block):
        share = block.shape[-1] // QUARTERS
        return jnp.concatenate(
            [block[:, part * share : (part + 1) * share] for part in range(QUARTERS)], axis=0
        )

    def unstacked(block):
        share = block.shape[0] // QUARTERS
        return jnp.concatenate(
            [block[part * share : (part + 1) * share] for part in range(QUARTERS)], axis=1
        )

    def take(picks, block):
        return lax.dot_general(
            picks, block, (((0,), (0,)), ((), ())), preferred_element_type=jnp.float32
        ).astype(jnp.bfloat16)

    def store_packed(sent, stage, block):
        share = block.shape[-1]
        for part in range(parts):
            sent[stage, :, :, part * share : (part + 1) * share] = block[
                part * tiles : (part + 1) * tiles
            ].reshape(per_group, BLOCK, share)

    def load_packed(landed, stage):
        block = landed[stage].reshape(tiles, landed.shape[-1])
        share = block.shape[-1] // parts
        return jnp.concatenate(
            [block[:, part * share : (part + 1) * share] for part in range(parts)], axis=0
        )

    def route(stage):
        if stage:
            column_landed(meta_send, meta_recv, meta_sems, stage).wait_recv()
        meta = meta_recv[stage].astype(jnp.float32)
        first = (row_names == meta[:, 0:1]).astype(jnp.float32)
        second = (row_names == meta[:, 1:2]).astype(jnp.float32)
        weights = first * (meta[:, 2:3] + meta[:, 3:4]) + second * (meta[:, 4:5] + meta[:, 5:6])
        both = first + second
        picks = jnp.concatenate([both * part for part in in_quarter], axis=0)
        weights = jnp.concatenate([weights * part for part in in_quarter], axis=0)
        high = weights.astype(jnp.bfloat16)
        picks_of[stage] = picks.astype(jnp.bfloat16)
        weights_of[stage] = (high, (weights - high.astype(jnp.float32)).astype(jnp.bfloat16))

    def spread(stage, picks, received, sent, landed, sems):
        block = stacked(received[stage].astype(jnp.float32)).astype(jnp.bfloat16)
        store_packed(sent, stage, take(picks, block))
        each_plane(lambda step: plane_copy(sent, landed, sems, stage, step).start())
        landed[stage, inner] = sent[stage, inner]

    def spread_tokens(stage):
        route(stage)
        if stage:
            column_landed(zsend, zrecv, z_sems, stage).wait_recv()
        spread(stage, picks_of[stage], zrecv, dsend, drecv, d_sems)

    def spread_nearer(first):
        stage = jnp.where(outer == first, 1, 2)
        near, far = (picks_of[1], picks_of[2]) if first else (picks_of[2], picks_of[1])
        picks = jnp.where(outer, near.astype(jnp.float32), far.astype(jnp.float32))
        column_landed(zsend, zrecv, z_sems, stage).wait_recv()
        spread(stage, picks.astype(jnp.bfloat16), zrecv, dsend, drecv, d_sems)

    def spread_heads(stage):
        if stage:
            column_landed(hsend, hrecv, h_sems, stage).wait_recv()
        spread(stage, picks_of[stage], hrecv, esend, erecv, e_sems)

    for small in smalls[4:]:
        small.wait()
    inputs = tokens[...].astype(jnp.float32)
    normed = rms(inputs, norm_gain[...]).astype(jnp.bfloat16)
    places = column(history_length[...].astype(jnp.float32))
    angles = places * inverse[...]
    cosine, sine = jnp.cos(angles), jnp.sin(angles)
    cosines = jnp.concatenate([cosine] * (2 * heads), axis=1)
    sines = jnp.concatenate([-sine, sine] * heads, axis=1)
    head_lane = lax.broadcasted_iota(jnp.int32, cosines.shape, 1)
    leading = lax.rem(head_lane, head_width) < half

    def rounded(weights):
        return dot(normed, weights[...]).astype(jnp.bfloat16).astype(jnp.float32)

    def rotated(values):
        partner = jnp.where(
            leading, jnp.roll(values, -half, axis=1), jnp.roll(values, half, axis=1)
        )
        return values * cosines + partner * sines

    def head_lanes(head):
        return slice(head * head_width, (head + 1) * head_width)

    with jax.named_scope("wait_q"):
        weight_copies[0].wait()
    queries = rotated(rounded(query_w))
    for head in range(heads):
        query_heads[head] = queries[:, head_lanes(head)]
    send_tokens(2, True)
    send_tokens(2, False)
    for block in range(2, blocks):
        if block == blocks - 2:
            weight_copies[3].start()
        state_in(block).start()
    with jax.named_scope("wait_k"):
        weight_copies[1].wait()
    keys = rotated(rounded(key_w)) * head_width ** (-0.5)
    with jax.named_scope("wait_v"):
        weight_copies[2].wait()
    values = rounded(value_w)
    products = keys * queries
    for head in range(heads):
        value_heads[head] = values[:, head_lanes(head)]
        overlap[head] = jnp.sum(products[:, head_lanes(head)], axis=1, keepdims=True)
    retain = [
        jnp.exp(jnp.full((1, head_width), -decay_rate[head], jnp.float32)) for head in range(heads)
    ]
    wide = (BLOCK, BLOCK * head_width)
    own = lax.broadcasted_iota(jnp.int32, wide, 0) == (
        lax.broadcasted_iota(jnp.int32, wide, 1) // head_width
    )

    def read(block, carry):
        state_in(block).wait()
        span = pl.ds(block * BLOCK, BLOCK)
        for head in range(heads):
            block_queries = query_heads[head, span, :]
            spread_queries = jnp.where(own, jnp.concatenate([block_queries] * BLOCK, axis=1), 0.0)
            high = spread_queries.astype(jnp.bfloat16).astype(jnp.float32)
            both = jnp.concatenate([high, spread_queries - high], axis=0).astype(jnp.bfloat16)
            old = state[span, head].reshape(BLOCK * head_width, head_width).astype(jnp.bfloat16)
            found = dot(both, old)
            reading[head, span, :] = (
                retain[head] * (found[:BLOCK] + found[BLOCK:])
                + overlap[head, span, :] * value_heads[head, span, :]
            )
        return carry

    def update(block, carry):
        span = pl.ds(block * BLOCK, BLOCK)
        for head in range(heads):
            lanes = slice(head * head_width, (head + 1) * head_width)
            block_values = value_heads[head, span, :]
            block_keys = key_columns[block, lanes, :]
            for index in range(BLOCK):
                sequence = block * BLOCK + index
                state[sequence, head] = (
                    retain[head] * state[sequence, head]
                    + block_keys[:, index : index + 1] * block_values[index : index + 1, :]
                )
        return carry

    def advance(first, last):
        with jax.named_scope(f"advance_{first}"):
            lax.fori_loop(first, last, update, 0)

    with jax.named_scope("spread_tokens_0"):
        spread_tokens(0)
    send_tokens(3, False)
    with jax.named_scope("read_a"):
        lax.fori_loop(0, blocks // 2, read, 0)
    send_tokens(1, True)
    with jax.named_scope("spread_near"):
        for stage in (1, 2):
            route(stage)
        spread_nearer(True)
    with jax.named_scope("read"):
        lax.fori_loop(blocks // 2, blocks, read, 0)
    for copy in weight_copies[4:] + loads:
        copy.start()
    with jax.named_scope("wait_g"):
        weight_copies[3].wait()
    gating = rounded(gate_w)
    read_heads = jnp.concatenate(
        [
            rms(
                reading[head],
                head_gain[:, head_lanes(head)],
            )
            for head in range(heads)
        ],
        axis=1,
    )
    mixed_heads = (read_heads * jax.nn.silu(gating)).astype(jnp.bfloat16)
    hsend[...] = dot(placing, mixed_heads).astype(jnp.bfloat16).reshape(hsend.shape)
    each_column(lambda step: column_copy(hsend, hrecv, h_sems, step).start())
    hrecv[0] = hsend[group]
    half_width = width // HALVES

    def run_expert(stage):
        plane_total(dsend, drecv, d_sems, stage).wait_recv()
        token_rows = unstacked(dot(packing, load_packed(drecv, stage)))
        plane_total(esend, erecv, e_sems, stage).wait_recv()
        head_rows = unstacked(dot(packing, load_packed(erecv, stage))).astype(jnp.bfloat16)
        block = (token_rows + dot(head_rows, out_w[...])).astype(jnp.bfloat16)
        block = rms(block.astype(jnp.float32), moe_gain[...]).astype(jnp.bfloat16)
        hidden = jax.nn.silu(dot(block, expert_gate_w[...])) * dot(block, expert_up_w[...])
        hidden = hidden.astype(jnp.bfloat16)
        for half in range(HALVES):
            lanes = slice(half * half_width, (half + 1) * half_width)
            block = dot(hidden, expert_down_w[:, lanes]).astype(jnp.bfloat16)
            store_packed(osend, stage * HALVES + half, take(packing, stacked(block)))
            if stage > 1:
                send_back(stage, half)
        if stage == 1:
            for half in range(HALVES):
                send_back(stage, half)

    def send_back(stage, half):
        index = stage * HALVES + half
        each_plane(lambda step: plane_copy(osend, orecv, o_sems, index, step).start())
        orecv[index, inner] = osend[index, inner]

    def combine(stage, half):
        index = stage * HALVES + half
        plane_total(osend, orecv, o_sems, index).wait_recv()
        block = load_packed(orecv, index)
        high, low = weights_of[stage]
        block = unstacked(dot(high, block) + dot(low, block)).astype(jnp.bfloat16)
        if stage:
            csend[stage, half] = block
            send_home(stage, half).start()
        else:
            crecv[group, half] = block

    def combine_all(stage):
        for half in range(HALVES):
            with jax.named_scope(f"combine_{stage}_{half}"):
                combine(stage, half)

    with jax.named_scope("spread_heads_0"):
        spread_heads(0)
    with jax.named_scope("spread_far"):
        spread_nearer(False)
    for block in range(blocks):
        key_columns[block] = keys[block * BLOCK : (block + 1) * BLOCK].T
    advance(0, blocks // 3)
    for stage in (2, 1):
        with jax.named_scope(f"spread_heads_{stage}"):
            spread_heads(stage)
    with jax.named_scope("spread_tokens_3"):
        spread_tokens(3)
    with jax.named_scope("wait_oe"):
        for copy in weight_copies[4:] + loads:
            copy.wait()

    with jax.named_scope("run_expert_0"):
        run_expert(0)
    with jax.named_scope("spread_heads_3"):
        spread_heads(3)
    for stage in (2, 1, 3):
        with jax.named_scope(f"run_expert_{stage}"):
            run_expert(stage)
    combine_all(2)
    for half in range(HALVES):
        send_back(0, half)
    combine_all(1)
    with jax.named_scope("mixed"):
        mixed = (inputs + dot(mixed_heads, out_w[...])).astype(jnp.bfloat16)
    advance(blocks // 3, blocks // 2)
    combine_all(3)
    advance(blocks // 2, 5 * blocks // 6)
    combine_all(0)
    advance(5 * blocks // 6, blocks)
    slot_across = lax.broadcasted_iota(jnp.int32, (seq_count, slots), 1).astype(jnp.float32)
    collecting = (slot_across == column(group_slot)).astype(jnp.float32).astype(jnp.bfloat16)
    for half in range(HALVES):
        lanes = slice(half * half_width, (half + 1) * half_width)
        with jax.named_scope(f"wait_home_{half}"):
            each_column(lambda step: home_landed(step, half).wait_recv())
        block = dot(collecting, crecv[:, half].reshape(slots, half_width))
        out[:, lanes] = (mixed[:, lanes].astype(jnp.float32) + block).astype(jnp.bfloat16)
    column_sent(meta_send, meta_recv, meta_sems).wait_send()
    column_sent(zsend, zrecv, z_sems).wait_send()
    column_sent(hsend, hrecv, h_sems).wait_send()
    column_sent(csend, crecv, c_sems).wait_send()
    plane_sent(dsend, drecv, d_sems).wait_send()
    plane_sent(esend, erecv, e_sems).wait_send()
    plane_sent(osend, orecv, o_sems).wait_send()


def finish_kernel(output, state, out, state_out, sem):
    blocks = sem.shape[0] - 1
    share = state.shape[0] // blocks
    copies = [pltpu.make_async_copy(output, out, sem.at[blocks])]
    for block in range(blocks):
        span = pl.ds(block * share, share)
        copies.append(pltpu.make_async_copy(state.at[span], state_out.at[span], sem.at[block]))
    for copy in copies:
        copy.start()
    for copy in copies:
        copy.wait()


def finish(output, new_state):
    vmem = pl.BlockSpec(memory_space=pltpu.VMEM)
    hbm = pl.BlockSpec(memory_space=pl.ANY)
    return pl.pallas_call(
        finish_kernel,
        name="finish",
        out_shape=(
            jax.ShapeDtypeStruct(output.shape, output.dtype),
            jax.ShapeDtypeStruct(new_state.shape, new_state.dtype),
        ),
        in_specs=[vmem, vmem],
        out_specs=(hbm, hbm),
        scratch_shapes=[pltpu.SemaphoreType.DMA((2 * new_state.shape[0] // BLOCK + 1,))],
        compiler_params=pltpu.CompilerParams(vmem_limit_bytes=4 * 1024 * 1024),
    )(output, new_state)


def local(
    tokens,
    history_length,
    norm_gain,
    w_query,
    w_key,
    w_value,
    w_gate,
    decay_rate,
    state,
    head_gain,
    w_out,
    moe_gain,
    route_weights,
    expert_group,
    expert_inner,
    expert_gate,
    expert_up,
    expert_down,
):
    experts = lax.axis_size("ep")
    per_group = experts // GROUPS
    heads = decay_rate.shape[0]
    seq_count, model_width = tokens.shape
    head_width = state.shape[-1]
    mixed_width = heads * head_width
    half = head_width // 2
    blocks = seq_count // BLOCK
    inverse = (10000.0 ** (-np.arange(half) / half)).astype(np.float32)
    capacity = max(2, 4 * seq_count // experts)
    group_rows = -(-min(seq_count, per_group * capacity // TOP_K) // 8) * 8
    capacity += capacity % 2
    packed = capacity * QUARTERS // BLOCK
    half_lanes = model_width // HALVES * packed // QUARTERS
    vmem = pl.BlockSpec(memory_space=pltpu.VMEM)
    smem = pl.BlockSpec(memory_space=pltpu.SMEM)
    hbm = pl.BlockSpec(memory_space=pl.ANY)
    dma = pltpu.SemaphoreType.DMA
    bf16, f32 = jnp.bfloat16, jnp.float32

    def column_buffer(lanes):
        return [pltpu.VMEM((GROUPS, group_rows, lanes), bf16)] * 2

    def plane_buffer(lanes):
        return [pltpu.VMEM((STAGES, per_group, BLOCK, lanes * packed // QUARTERS), bf16)] * 2

    weights = (w_query, w_key, w_value, w_gate, w_out, expert_gate[0], expert_up[0], expert_down[0])
    state_bytes = state.size // head_width * max(head_width, 128) * 4

    smalls = (
        tokens,
        history_length.reshape(1, -1),
        inverse.reshape(1, -1),
        norm_gain.reshape(1, -1),
        head_gain.reshape(1, -1),
        moe_gain.reshape(1, -1),
        expert_group.reshape(1, -1),
        expert_inner.T,
        route_weights.T,
    )

    def kernel(*refs):
        layer_kernel(per_group, capacity, *refs)

    output, new_state = pl.pallas_call(
        kernel,
        name="layer",
        out_shape=(
            pltpu.VMEM((seq_count, model_width), bf16),
            pltpu.VMEM(state.shape, f32),
        ),
        in_specs=[smem] + [hbm] * 18,
        out_specs=(vmem, vmem),
        scratch_shapes=[pltpu.VMEM(weight.shape, bf16) for weight in weights]
        + [pltpu.VMEM(small.shape, small.dtype) for small in smalls]
        + [
            pltpu.VMEM((blocks, mixed_width, BLOCK), f32),
            pltpu.VMEM((heads, seq_count, head_width), f32),
            pltpu.VMEM((heads, seq_count, head_width), f32),
            pltpu.VMEM((heads, seq_count, head_width), f32),
            pltpu.VMEM((heads, seq_count, 1), f32),
        ]
        + column_buffer(128)
        + column_buffer(model_width)
        + column_buffer(mixed_width)
        + plane_buffer(model_width)
        + plane_buffer(mixed_width)
        + [pltpu.VMEM((STAGES * HALVES, per_group, BLOCK, half_lanes), bf16)] * 2
        + [pltpu.VMEM((GROUPS, HALVES, group_rows, model_width // HALVES), bf16)] * 2
        + [
            dma((9,)),
            dma((5,)),
            dma((blocks,)),
            dma((3,)),
            dma((GROUPS,)),
            dma((GROUPS,)),
            dma((GROUPS,)),
            dma((STAGES + 1,)),
            dma((STAGES + 1,)),
            dma((STAGES * HALVES + 1,)),
            dma((GROUPS * HALVES,)),
        ],
        compiler_params=pltpu.CompilerParams(
            collective_id=0,
            has_side_effects=True,
            vmem_limit_bytes=63 * 1024 * 1024 - state_bytes,
        ),
    )(
        decay_rate,
        *smalls,
        w_query,
        w_key,
        w_value,
        w_gate,
        w_out,
        state,
        expert_gate[0],
        expert_up[0],
        expert_down[0],
    )
    return finish(output, new_state)


def solution(mesh):
    return jax.shard_map(
        local,
        mesh=mesh,
        in_specs=(
            P("ep", None),
            P("ep"),
            P(),
            P(),
            P(),
            P(),
            P(),
            P(),
            P("ep", None, None, None),
            P(),
            P(),
            P(),
            P("ep", None),
            P("ep"),
            P("ep", None),
            P("ep", None, None),
            P("ep", None, None),
            P("ep", None, None),
        ),
        out_specs=(P("ep", None), P("ep", None, None, None)),
        check_vma=False,
    )
```

```python
import jax
import jax.numpy as jnp
import numpy as np
from jax import lax
from jax.experimental import pallas as pl
from jax.experimental.pallas import tpu as pltpu
from jax.sharding import PartitionSpec as P

GROUPS = 4
TOP_K = 2


epsilon = 1e-06


BLOCK = 8


MESH = pl.DeviceIdType.MESH
STAGES = GROUPS
QUARTERS = 4
HALVES = 2
ORDER = (2, 3, 1)


def dot(a, b):
    return jnp.dot(a, b, preferred_element_type=jnp.float32)


def rms(values, gains):
    mean = jnp.mean(values * values, axis=-1, keepdims=True)
    return values * lax.rsqrt(mean + epsilon) * gains


def layer_kernel(
    per_group,
    capacity,
    decay_rate,
    tokens_hbm,
    history_length_hbm,
    inverse_hbm,
    norm_gain_hbm,
    head_gain_hbm,
    moe_gain_hbm,
    expert_group_hbm,
    expert_inner_hbm,
    route_weights_hbm,
    query_hbm,
    key_hbm,
    value_hbm,
    gate_hbm,
    out_hbm,
    state_hbm,
    expert_gate_hbm,
    expert_up_hbm,
    expert_down_hbm,
    out,
    state,
    query_w,
    key_w,
    value_w,
    gate_w,
    out_w,
    expert_gate_w,
    expert_up_w,
    expert_down_w,
    tokens,
    history_length,
    inverse,
    norm_gain,
    head_gain,
    moe_gain,
    expert_group,
    expert_inner,
    route_weights,
    key_columns,
    value_heads,
    query_heads,
    reading,
    overlap,
    meta_send,
    meta_recv,
    zsend,
    zrecv,
    hsend,
    hrecv,
    dsend,
    drecv,
    esend,
    erecv,
    osend,
    orecv,
    csend,
    crecv,
    small_sem,
    weight_sem,
    in_sem,
    load_sem,
    meta_sems,
    z_sems,
    h_sems,
    d_sems,
    e_sems,
    o_sems,
    c_sems,
):
    device = lax.axis_index("ep")
    group = device // per_group
    inner = device % per_group
    seq_count, width = tokens.shape
    group_rows = zsend.shape[1]
    slots = GROUPS * group_rows
    rows = per_group * capacity
    tiles = per_group * BLOCK
    parts = capacity * QUARTERS // BLOCK
    heads, head_width = state.shape[1], state.shape[-1]
    half = head_width // 2
    blocks = seq_count // BLOCK

    side = group // 2
    within = group * (GROUPS - 1 - group) // 2
    others = {1: group + 1 - 2 * (group % 2), 2: 3 * (1 - side), 3: 2 - side}
    landing = {1: 1, 2: 2 + within, 3: 2 + within}

    def column_peer(step):
        return others[step], others[step] * per_group + inner

    def plane_peer(step):
        other = lax.rem(inner + step, per_group)
        return other, group * per_group + other

    def remote(source, target, send_sem, recv_sem, peer):
        return pltpu.make_async_remote_copy(
            src_ref=source,
            dst_ref=target,
            send_sem=send_sem,
            recv_sem=recv_sem,
            device_id=(peer,),
            device_id_type=MESH,
        )

    def column_copy(source, target, sems, step):
        other, peer = column_peer(step)
        place = landing[step]
        return remote(source.at[other], target.at[place], sems.at[0], sems.at[place], peer)

    def column_landed(source, target, sems, step):
        return remote(source.at[0], target.at[step], sems.at[0], sems.at[step], column_peer(1)[1])

    def column_sent(source, target, sems):
        others = pl.ds(1, GROUPS - 1)
        return remote(source.at[others], target.at[others], sems.at[0], sems.at[1], column_peer(1)[1])

    def send_home(step, half):
        return remote(
            csend.at[step, half],
            crecv.at[group, half],
            c_sems.at[0],
            c_sems.at[landing[step] * HALVES + half],
            column_peer(step)[1],
        )

    def home_landed(step, half):
        return remote(
            csend.at[step, half],
            crecv.at[step, half],
            c_sems.at[0],
            c_sems.at[step * HALVES + half],
            column_peer(step)[1],
        )

    def plane_copy(source, target, sems, stage, step):
        other, peer = plane_peer(step)
        return remote(
            source.at[stage, other],
            target.at[stage, inner],
            sems.at[0],
            sems.at[stage + 1],
            peer,
        )

    def plane_total(source, target, sems, stage):
        others = pl.ds(0, per_group - 1)
        return remote(
            source.at[stage, others],
            target.at[stage, others],
            sems.at[0],
            sems.at[stage + 1],
            plane_peer(1)[1],
        )

    def plane_sent(source, target, sems):
        others = pl.ds(0, per_group - 1)
        return remote(
            source.at[:, others], target.at[:, others], sems.at[0], sems.at[1], plane_peer(1)[1]
        )

    def each_column(act):
        for step in ORDER:
            act(step)

    def each_plane(act):
        def body(step, carry):
            act(step)
            return carry

        lax.fori_loop(1, per_group, body, 0)

    def load_all(pairs, sem):
        return [
            pltpu.make_async_copy(source, target, sem.at[index])
            for index, (source, target) in enumerate(pairs)
        ]

    barrier = pltpu.get_barrier_semaphore()

    def greet_column(step):
        pl.semaphore_signal(barrier, inc=1, device_id=(column_peer(step)[1],), device_id_type=MESH)

    def greet_plane(step):
        pl.semaphore_signal(barrier, inc=1, device_id=(plane_peer(step)[1],), device_id_type=MESH)

    smalls = load_all(
        (
            (expert_group_hbm, expert_group),
            (tokens_hbm, tokens),
            (expert_inner_hbm, expert_inner),
            (route_weights_hbm, route_weights),
            (norm_gain_hbm, norm_gain),
            (history_length_hbm, history_length),
            (inverse_hbm, inverse),
            (head_gain_hbm, head_gain),
            (moe_gain_hbm, moe_gain),
        ),
        small_sem,
    )
    weight_copies = load_all(
        (
            (query_hbm, query_w),
            (key_hbm, key_w),
            (value_hbm, value_w),
            (gate_hbm, gate_w),
            (out_hbm, out_w),
        ),
        weight_sem,
    )
    loads = load_all(
        (
            (expert_gate_hbm, expert_gate_w),
            (expert_up_hbm, expert_up_w),
            (expert_down_hbm, expert_down_w),
        ),
        load_sem,
    )

    def state_in(block):
        span = pl.ds(block * BLOCK, BLOCK)
        return pltpu.make_async_copy(state_hbm.at[span], state.at[span], in_sem.at[block])

    for copy in smalls + weight_copies[:1]:
        copy.start()
    each_column(greet_column)
    each_plane(greet_plane)
    for copy in weight_copies[1:3]:
        copy.start()

    square = (seq_count, seq_count)
    above = lax.broadcasted_iota(jnp.int32, square, 0)
    across = lax.broadcasted_iota(jnp.int32, square, 1)

    def column(row):
        return jnp.sum(jnp.where(above == across, row, 0.0), axis=1, keepdims=True)

    def earlier(columns, row):
        matched = sum((values == row).astype(jnp.float32) for values in columns)
        return jnp.sum(jnp.where(above < across, matched, 0.0), axis=0, keepdims=True)

    smalls[0].wait()
    group_row = expert_group[...].astype(jnp.float32)
    group_slot = group_row * group_rows + earlier([column(group_row)], group_row)
    slot_above = lax.broadcasted_iota(jnp.int32, (slots, seq_count), 0).astype(jnp.float32)
    placing = (slot_above == group_slot).astype(jnp.float32).astype(jnp.bfloat16)
    smalls[1].wait()
    zsend[...] = dot(placing, tokens[...]).astype(jnp.bfloat16).reshape(zsend.shape)
    with jax.named_scope("barrier"):
        pl.semaphore_wait(barrier, GROUPS - 1 + per_group - 1)
    outer = within == 0

    def send_tokens(stage, held):
        @pl.when(outer if held else jnp.logical_not(outer))
        def start():
            column_copy(zsend, zrecv, z_sems, stage).start()

    send_tokens(3, True)
    send_tokens(1, False)
    for block in range(2):
        state_in(block).start()
    for small in smalls[2:4]:
        small.wait()
    inner_rows = [expert_inner[choice : choice + 1, :].astype(jnp.float32) for choice in (0, 1)]
    expert_rows = [group_row * per_group + row for row in inner_rows]
    expert_columns = [column(row) for row in expert_rows]
    lanes = []
    for choice in (0, 1):
        slot = earlier(expert_columns, expert_rows[choice])
        lanes.append(column(inner_rows[choice] * capacity + slot + 1.0))
    for choice in (0, 1):
        weight = column(route_weights[choice : choice + 1, :])
        high = weight.astype(jnp.bfloat16).astype(jnp.float32)
        lanes += [high, weight - high]
    lane = lax.broadcasted_iota(jnp.int32, (seq_count, meta_send.shape[-1]), 1)
    token_meta = jnp.zeros(lane.shape, jnp.float32)
    for index, value in enumerate(lanes):
        token_meta = jnp.where(lane == index, value, token_meta)
    meta = dot(placing, token_meta.astype(jnp.bfloat16)).astype(jnp.bfloat16)
    meta_send[...] = meta.reshape(meta_send.shape)
    each_column(lambda step: column_copy(meta_send, meta_recv, meta_sems, step).start())
    meta_recv[0] = meta_send[group]
    zrecv[0] = zsend[group]

    def packed_places(shape, axis):
        index = lax.broadcasted_iota(jnp.int32, shape, axis)
        part = sum((index >= tiles * bound).astype(jnp.int32) for bound in range(1, parts))
        index = index - part * tiles
        place = (index & (BLOCK - 1)) * parts + part
        return (index >> 3) * capacity + (place >> 2), place & (QUARTERS - 1)

    packed_rows, packed_quarter = packed_places((1, parts * tiles), 1)
    row_names = packed_rows.astype(jnp.float32) + 1.0
    in_quarter = [(packed_quarter == part).astype(jnp.float32) for part in range(QUARTERS)]
    row_number = lax.broadcasted_iota(jnp.int32, (rows, parts * tiles), 0)
    same_row = (row_number == packed_rows).astype(jnp.float32)
    packing = jnp.concatenate([same_row * part for part in in_quarter], axis=0).astype(jnp.bfloat16)
    picks_of = {}
    weights_of = {}

    def stacked(block):
        share = block.shape[-1] // QUARTERS
        return jnp.concatenate(
            [block[:, part * share : (part + 1) * share] for part in range(QUARTERS)], axis=0
        )

    def unstacked(block):
        share = block.shape[0] // QUARTERS
        return jnp.concatenate(
            [block[part * share : (part + 1) * share] for part in range(QUARTERS)], axis=1
        )

    def take(picks, block):
        return lax.dot_general(
            picks, block, (((0,), (0,)), ((), ())), preferred_element_type=jnp.float32
        ).astype(jnp.bfloat16)

    def store_packed(sent, stage, block):
        share = block.shape[-1]
        for part in range(parts):
            sent[stage, :, :, part * share : (part + 1) * share] = block[
                part * tiles : (part + 1) * tiles
            ].reshape(per_group, BLOCK, share)

    def load_packed(landed, stage):
        block = landed[stage].reshape(tiles, landed.shape[-1])
        share = block.shape[-1] // parts
        return jnp.concatenate(
            [block[:, part * share : (part + 1) * share] for part in range(parts)], axis=0
        )

    def route(stage):
        if stage:
            column_landed(meta_send, meta_recv, meta_sems, stage).wait_recv()
        meta = meta_recv[stage].astype(jnp.float32)
        first = (row_names == meta[:, 0:1]).astype(jnp.float32)
        second = (row_names == meta[:, 1:2]).astype(jnp.float32)
        weights = first * (meta[:, 2:3] + meta[:, 3:4]) + second * (meta[:, 4:5] + meta[:, 5:6])
        both = first + second
        picks = jnp.concatenate([both * part for part in in_quarter], axis=0)
        weights = jnp.concatenate([weights * part for part in in_quarter], axis=0)
        high = weights.astype(jnp.bfloat16)
        picks_of[stage] = picks.astype(jnp.bfloat16)
        weights_of[stage] = (high, (weights - high.astype(jnp.float32)).astype(jnp.bfloat16))

    def spread(stage, picks, received, sent, landed, sems):
        block = stacked(received[stage].astype(jnp.float32)).astype(jnp.bfloat16)
        store_packed(sent, stage, take(picks, block))
        each_plane(lambda step: plane_copy(sent, landed, sems, stage, step).start())
        landed[stage, inner] = sent[stage, inner]

    def spread_tokens(stage):
        route(stage)
        if stage:
            column_landed(zsend, zrecv, z_sems, stage).wait_recv()
        spread(stage, picks_of[stage], zrecv, dsend, drecv, d_sems)

    def spread_nearer(first):
        stage = jnp.where(outer == first, 1, 2)
        near, far = (picks_of[1], picks_of[2]) if first else (picks_of[2], picks_of[1])
        picks = jnp.where(outer, near.astype(jnp.float32), far.astype(jnp.float32))
        column_landed(zsend, zrecv, z_sems, stage).wait_recv()
        spread(stage, picks.astype(jnp.bfloat16), zrecv, dsend, drecv, d_sems)

    def spread_heads(stage):
        if stage:
            column_landed(hsend, hrecv, h_sems, stage).wait_recv()
        spread(stage, picks_of[stage], hrecv, esend, erecv, e_sems)

    for small in smalls[4:]:
        small.wait()
    inputs = tokens[...].astype(jnp.float32)
    normed = rms(inputs, norm_gain[...]).astype(jnp.bfloat16)
    places = column(history_length[...].astype(jnp.float32))
    angles = places * inverse[...]
    cosine, sine = jnp.cos(angles), jnp.sin(angles)
    cosines = jnp.concatenate([cosine] * (2 * heads), axis=1)
    sines = jnp.concatenate([-sine, sine] * heads, axis=1)
    head_lane = lax.broadcasted_iota(jnp.int32, cosines.shape, 1)
    leading = lax.rem(head_lane, head_width) < half

    def rounded(weights):
        return dot(normed, weights[...]).astype(jnp.bfloat16).astype(jnp.float32)

    def rotated(values):
        partner = jnp.where(
            leading, jnp.roll(values, -half, axis=1), jnp.roll(values, half, axis=1)
        )
        return values * cosines + partner * sines

    def head_lanes(head):
        return slice(head * head_width, (head + 1) * head_width)

    with jax.named_scope("wait_q"):
        weight_copies[0].wait()
    queries = rotated(rounded(query_w))
    for head in range(heads):
        query_heads[head] = queries[:, head_lanes(head)]
    send_tokens(2, True)
    send_tokens(2, False)
    for block in range(2, blocks):
        if block == blocks - 2:
            weight_copies[3].start()
        state_in(block).start()
    with jax.named_scope("wait_k"):
        weight_copies[1].wait()
    keys = rotated(rounded(key_w)) * head_width ** (-0.5)
    with jax.named_scope("wait_v"):
        weight_copies[2].wait()
    values = rounded(value_w)
    products = keys * queries
    for head in range(heads):
        value_heads[head] = values[:, head_lanes(head)]
        overlap[head] = jnp.sum(products[:, head_lanes(head)], axis=1, keepdims=True)
    retain = [
        jnp.exp(jnp.full((1, head_width), -decay_rate[head], jnp.float32)) for head in range(heads)
    ]
    wide = (BLOCK, BLOCK * head_width)
    own = lax.broadcasted_iota(jnp.int32, wide, 0) == (
        lax.broadcasted_iota(jnp.int32, wide, 1) // head_width
    )

    def read(block, carry):
        state_in(block).wait()
        span = pl.ds(block * BLOCK, BLOCK)
        for head in range(heads):
            block_queries = query_heads[head, span, :]
            spread_queries = jnp.where(own, jnp.concatenate([block_queries] * BLOCK, axis=1), 0.0)
            high = spread_queries.astype(jnp.bfloat16).astype(jnp.float32)
            both = jnp.concatenate([high, spread_queries - high], axis=0).astype(jnp.bfloat16)
            old = state[span, head].reshape(BLOCK * head_width, head_width).astype(jnp.bfloat16)
            found = dot(both, old)
            reading[head, span, :] = (
                retain[head] * (found[:BLOCK] + found[BLOCK:])
                + overlap[head, span, :] * value_heads[head, span, :]
            )
        return carry

    def update(block, carry):
        span = pl.ds(block * BLOCK, BLOCK)
        for head in range(heads):
            lanes = slice(head * head_width, (head + 1) * head_width)
            block_values = value_heads[head, span, :]
            block_keys = key_columns[block, lanes, :]
            for index in range(BLOCK):
                sequence = block * BLOCK + index
                state[sequence, head] = (
                    retain[head] * state[sequence, head]
                    + block_keys[:, index : index + 1] * block_values[index : index + 1, :]
                )
        return carry

    def advance(first, last):
        with jax.named_scope(f"advance_{first}"):
            lax.fori_loop(first, last, update, 0)

    with jax.named_scope("spread_tokens_0"):
        spread_tokens(0)
    send_tokens(3, False)
    with jax.named_scope("read_a"):
        lax.fori_loop(0, blocks // 2, read, 0)
    send_tokens(1, True)
    with jax.named_scope("spread_near"):
        for stage in (1, 2):
            route(stage)
        spread_nearer(True)
    with jax.named_scope("read"):
        lax.fori_loop(blocks // 2, blocks, read, 0)
    for copy in weight_copies[4:] + loads:
        copy.start()
    with jax.named_scope("wait_g"):
        weight_copies[3].wait()
    gating = rounded(gate_w)
    read_heads = jnp.concatenate(
        [
            rms(
                reading[head],
                head_gain[:, head_lanes(head)],
            )
            for head in range(heads)
        ],
        axis=1,
    )
    mixed_heads = (read_heads * jax.nn.silu(gating)).astype(jnp.bfloat16)
    hsend[...] = dot(placing, mixed_heads).astype(jnp.bfloat16).reshape(hsend.shape)
    each_column(lambda step: column_copy(hsend, hrecv, h_sems, step).start())
    hrecv[0] = hsend[group]
    half_width = width // HALVES

    def run_expert(*stages):
        token_rows, head_rows = [], []
        for stage in stages:
            plane_total(dsend, drecv, d_sems, stage).wait_recv()
            token_rows.append(unstacked(dot(packing, load_packed(drecv, stage))))
        for stage in stages:
            plane_total(esend, erecv, e_sems, stage).wait_recv()
            head_rows.append(unstacked(dot(packing, load_packed(erecv, stage))))
        head_rows = jnp.concatenate(head_rows, axis=0).astype(jnp.bfloat16)
        token_rows = jnp.concatenate(token_rows, axis=0)
        block = (token_rows + dot(head_rows, out_w[...])).astype(jnp.bfloat16)
        block = rms(block.astype(jnp.float32), moe_gain[...]).astype(jnp.bfloat16)
        hidden = jax.nn.silu(dot(block, expert_gate_w[...])) * dot(block, expert_up_w[...])
        hidden = hidden.astype(jnp.bfloat16)
        for half in range(HALVES):
            lanes = slice(half * half_width, (half + 1) * half_width)
            block = dot(hidden, expert_down_w[:, lanes])
            for place, stage in enumerate(stages):
                share = block[place * rows : (place + 1) * rows].astype(jnp.bfloat16)
                store_packed(osend, stage * HALVES + half, take(packing, stacked(share)))
            if stages[0]:
                for stage in stages:
                    send_back(stage, half)

    def send_back(stage, half):
        index = stage * HALVES + half
        each_plane(lambda step: plane_copy(osend, orecv, o_sems, index, step).start())
        orecv[index, inner] = osend[index, inner]

    def combine(stage, half):
        index = stage * HALVES + half
        plane_total(osend, orecv, o_sems, index).wait_recv()
        block = load_packed(orecv, index)
        high, low = weights_of[stage]
        block = unstacked(dot(high, block) + dot(low, block)).astype(jnp.bfloat16)
        if stage:
            csend[stage, half] = block
            send_home(stage, half).start()
        else:
            crecv[group, half] = block

    def combine_all(stage):
        for half in range(HALVES):
            with jax.named_scope(f"combine_{stage}_{half}"):
                combine(stage, half)

    with jax.named_scope("spread_heads_0"):
        spread_heads(0)
    with jax.named_scope("spread_far"):
        spread_nearer(False)
    for block in range(blocks):
        key_columns[block] = keys[block * BLOCK : (block + 1) * BLOCK].T
    advance(0, blocks // 3)
    for stage in (2, 1):
        with jax.named_scope(f"spread_heads_{stage}"):
            spread_heads(stage)
    with jax.named_scope("spread_tokens_3"):
        spread_tokens(3)
    with jax.named_scope("wait_oe"):
        for copy in weight_copies[4:] + loads:
            copy.wait()

    with jax.named_scope("run_expert_0"):
        run_expert(0)
    with jax.named_scope("spread_heads_3"):
        spread_heads(3)
    with jax.named_scope("run_expert_2"):
        run_expert(2)
    with jax.named_scope("run_expert_31"):
        run_expert(1, 3)
    combine_all(2)
    for half in range(HALVES):
        send_back(0, half)
    with jax.named_scope("mixed"):
        mixed = (inputs + dot(mixed_heads, out_w[...])).astype(jnp.bfloat16)
    advance(blocks // 3, blocks // 2)
    for half in range(HALVES):
        for stage in (1, 3):
            with jax.named_scope(f"combine_{stage}_{half}"):
                combine(stage, half)
        advance((3 + half) * blocks // 6, (4 + half) * blocks // 6)
    combine_all(0)
    advance(5 * blocks // 6, blocks)
    slot_across = lax.broadcasted_iota(jnp.int32, (seq_count, slots), 1).astype(jnp.float32)
    collecting = (slot_across == column(group_slot)).astype(jnp.float32).astype(jnp.bfloat16)
    for half in range(HALVES):
        lanes = slice(half * half_width, (half + 1) * half_width)
        with jax.named_scope(f"wait_home_{half}"):
            each_column(lambda step: home_landed(step, half).wait_recv())
        block = dot(collecting, crecv[:, half].reshape(slots, half_width))
        out[:, lanes] = (mixed[:, lanes].astype(jnp.float32) + block).astype(jnp.bfloat16)
    column_sent(meta_send, meta_recv, meta_sems).wait_send()
    column_sent(zsend, zrecv, z_sems).wait_send()
    column_sent(hsend, hrecv, h_sems).wait_send()
    column_sent(csend, crecv, c_sems).wait_send()
    plane_sent(dsend, drecv, d_sems).wait_send()
    plane_sent(esend, erecv, e_sems).wait_send()
    plane_sent(osend, orecv, o_sems).wait_send()


def finish_kernel(output, state, out, state_out, sem):
    blocks = sem.shape[0] - 1
    share = state.shape[0] // blocks
    copies = [pltpu.make_async_copy(output, out, sem.at[blocks])]
    for block in range(blocks):
        span = pl.ds(block * share, share)
        copies.append(pltpu.make_async_copy(state.at[span], state_out.at[span], sem.at[block]))
    for copy in copies:
        copy.start()
    for copy in copies:
        copy.wait()


def finish(output, new_state):
    vmem = pl.BlockSpec(memory_space=pltpu.VMEM)
    hbm = pl.BlockSpec(memory_space=pl.ANY)
    return pl.pallas_call(
        finish_kernel,
        name="finish",
        out_shape=(
            jax.ShapeDtypeStruct(output.shape, output.dtype),
            jax.ShapeDtypeStruct(new_state.shape, new_state.dtype),
        ),
        in_specs=[vmem, vmem],
        out_specs=(hbm, hbm),
        scratch_shapes=[pltpu.SemaphoreType.DMA((2 * new_state.shape[0] // BLOCK + 1,))],
        compiler_params=pltpu.CompilerParams(vmem_limit_bytes=4 * 1024 * 1024),
    )(output, new_state)


def local(
    tokens,
    history_length,
    norm_gain,
    w_query,
    w_key,
    w_value,
    w_gate,
    decay_rate,
    state,
    head_gain,
    w_out,
    moe_gain,
    route_weights,
    expert_group,
    expert_inner,
    expert_gate,
    expert_up,
    expert_down,
):
    experts = lax.axis_size("ep")
    per_group = experts // GROUPS
    heads = decay_rate.shape[0]
    seq_count, model_width = tokens.shape
    head_width = state.shape[-1]
    mixed_width = heads * head_width
    half = head_width // 2
    blocks = seq_count // BLOCK
    inverse = (10000.0 ** (-np.arange(half) / half)).astype(np.float32)
    capacity = max(2, 4 * seq_count // experts)
    group_rows = -(-min(seq_count, per_group * capacity // TOP_K) // 8) * 8
    capacity += capacity % 2
    packed = capacity * QUARTERS // BLOCK
    half_lanes = model_width // HALVES * packed // QUARTERS
    vmem = pl.BlockSpec(memory_space=pltpu.VMEM)
    smem = pl.BlockSpec(memory_space=pltpu.SMEM)
    hbm = pl.BlockSpec(memory_space=pl.ANY)
    dma = pltpu.SemaphoreType.DMA
    bf16, f32 = jnp.bfloat16, jnp.float32

    def column_buffer(lanes):
        return [pltpu.VMEM((GROUPS, group_rows, lanes), bf16)] * 2

    def plane_buffer(lanes):
        return [pltpu.VMEM((STAGES, per_group, BLOCK, lanes * packed // QUARTERS), bf16)] * 2

    weights = (w_query, w_key, w_value, w_gate, w_out, expert_gate[0], expert_up[0], expert_down[0])
    state_bytes = state.size // head_width * max(head_width, 128) * 4

    smalls = (
        tokens,
        history_length.reshape(1, -1),
        inverse.reshape(1, -1),
        norm_gain.reshape(1, -1),
        head_gain.reshape(1, -1),
        moe_gain.reshape(1, -1),
        expert_group.reshape(1, -1),
        expert_inner.T,
        route_weights.T,
    )

    def kernel(*refs):
        layer_kernel(per_group, capacity, *refs)

    output, new_state = pl.pallas_call(
        kernel,
        name="layer",
        out_shape=(
            pltpu.VMEM((seq_count, model_width), bf16),
            pltpu.VMEM(state.shape, f32),
        ),
        in_specs=[smem] + [hbm] * 18,
        out_specs=(vmem, vmem),
        scratch_shapes=[pltpu.VMEM(weight.shape, bf16) for weight in weights]
        + [pltpu.VMEM(small.shape, small.dtype) for small in smalls]
        + [
            pltpu.VMEM((blocks, mixed_width, BLOCK), f32),
            pltpu.VMEM((heads, seq_count, head_width), f32),
            pltpu.VMEM((heads, seq_count, head_width), f32),
            pltpu.VMEM((heads, seq_count, head_width), f32),
            pltpu.VMEM((heads, seq_count, 1), f32),
        ]
        + column_buffer(128)
        + column_buffer(model_width)
        + column_buffer(mixed_width)
        + plane_buffer(model_width)
        + plane_buffer(mixed_width)
        + [pltpu.VMEM((STAGES * HALVES, per_group, BLOCK, half_lanes), bf16)] * 2
        + [pltpu.VMEM((GROUPS, HALVES, group_rows, model_width // HALVES), bf16)] * 2
        + [
            dma((9,)),
            dma((5,)),
            dma((blocks,)),
            dma((3,)),
            dma((GROUPS,)),
            dma((GROUPS,)),
            dma((GROUPS,)),
            dma((STAGES + 1,)),
            dma((STAGES + 1,)),
            dma((STAGES * HALVES + 1,)),
            dma((GROUPS * HALVES,)),
        ],
        compiler_params=pltpu.CompilerParams(
            collective_id=0,
            has_side_effects=True,
            vmem_limit_bytes=63 * 1024 * 1024 - state_bytes,
        ),
    )(
        decay_rate,
        *smalls,
        w_query,
        w_key,
        w_value,
        w_gate,
        w_out,
        state,
        expert_gate[0],
        expert_up[0],
        expert_down[0],
    )
    return finish(output, new_state)


def solution(mesh):
    return jax.shard_map(
        local,
        mesh=mesh,
        in_specs=(
            P("ep", None),
            P("ep"),
            P(),
            P(),
            P(),
            P(),
            P(),
            P(),
            P("ep", None, None, None),
            P(),
            P(),
            P(),
            P("ep", None),
            P("ep"),
            P("ep", None),
            P("ep", None, None),
            P("ep", None, None),
            P("ep", None, None),
        ),
        out_specs=(P("ep", None), P("ep", None, None, None)),
        check_vma=False,
    )
```

```python
import jax
import jax.numpy as jnp
import numpy as np
from jax import lax
from jax.experimental import pallas as pl
from jax.experimental.pallas import tpu as pltpu
from jax.sharding import PartitionSpec as P

GROUPS = 4
TOP_K = 2


epsilon = 1e-06


BLOCK = 8


MESH = pl.DeviceIdType.MESH
STAGES = GROUPS
QUARTERS = 4
HALVES = 2
ORDER = (2, 3, 1)


def dot(a, b):
    return jnp.dot(a, b, preferred_element_type=jnp.float32)


def rms(values, gains):
    mean = jnp.mean(values * values, axis=-1, keepdims=True)
    return values * lax.rsqrt(mean + epsilon) * gains


def layer_kernel(
    per_group,
    capacity,
    decay_rate,
    tokens_hbm,
    history_length_hbm,
    inverse_hbm,
    norm_gain_hbm,
    head_gain_hbm,
    moe_gain_hbm,
    expert_group_hbm,
    expert_inner_hbm,
    route_weights_hbm,
    query_hbm,
    key_hbm,
    value_hbm,
    gate_hbm,
    out_hbm,
    state_hbm,
    expert_gate_hbm,
    expert_up_hbm,
    expert_down_hbm,
    out,
    state,
    query_w,
    key_w,
    value_w,
    gate_w,
    out_w,
    expert_gate_w,
    expert_up_w,
    expert_down_w,
    tokens,
    history_length,
    inverse,
    norm_gain,
    head_gain,
    moe_gain,
    expert_group,
    expert_inner,
    route_weights,
    key_columns,
    value_heads,
    query_heads,
    reading,
    overlap,
    meta_send,
    meta_recv,
    zsend,
    zrecv,
    hsend,
    hrecv,
    dsend,
    drecv,
    esend,
    erecv,
    osend,
    orecv,
    csend,
    crecv,
    small_sem,
    weight_sem,
    in_sem,
    load_sem,
    meta_sems,
    z_sems,
    h_sems,
    d_sems,
    e_sems,
    o_sems,
    c_sems,
):
    device = lax.axis_index("ep")
    group = device // per_group
    inner = device % per_group
    seq_count, width = tokens.shape
    group_rows = zsend.shape[1]
    slots = GROUPS * group_rows
    rows = per_group * capacity
    tiles = per_group * BLOCK
    parts = capacity * QUARTERS // BLOCK
    heads, head_width = state.shape[1], state.shape[-1]
    half = head_width // 2
    blocks = seq_count // BLOCK

    side = group // 2
    within = group * (GROUPS - 1 - group) // 2
    others = {1: group + 1 - 2 * (group % 2), 2: 3 * (1 - side), 3: 2 - side}
    landing = {1: 1, 2: 2 + within, 3: 2 + within}

    def column_peer(step):
        return others[step], others[step] * per_group + inner

    def plane_peer(step):
        other = lax.rem(inner + step, per_group)
        return other, group * per_group + other

    def remote(source, target, send_sem, recv_sem, peer):
        return pltpu.make_async_remote_copy(
            src_ref=source,
            dst_ref=target,
            send_sem=send_sem,
            recv_sem=recv_sem,
            device_id=(peer,),
            device_id_type=MESH,
        )

    def column_copy(source, target, sems, step):
        other, peer = column_peer(step)
        place = landing[step]
        return remote(source.at[other], target.at[place], sems.at[0], sems.at[place], peer)

    def column_landed(source, target, sems, step):
        return remote(source.at[0], target.at[step], sems.at[0], sems.at[step], column_peer(1)[1])

    def column_sent(source, target, sems):
        others = pl.ds(1, GROUPS - 1)
        return remote(source.at[others], target.at[others], sems.at[0], sems.at[1], column_peer(1)[1])

    def send_home(step, half):
        return remote(
            csend.at[step, half],
            crecv.at[group, half],
            c_sems.at[0],
            c_sems.at[landing[step] * HALVES + half],
            column_peer(step)[1],
        )

    def home_landed(step, half):
        return remote(
            csend.at[step, half],
            crecv.at[step, half],
            c_sems.at[0],
            c_sems.at[step * HALVES + half],
            column_peer(step)[1],
        )

    def plane_copy(source, target, sems, stage, step):
        other, peer = plane_peer(step)
        return remote(
            source.at[stage, other],
            target.at[stage, inner],
            sems.at[0],
            sems.at[stage + 1],
            peer,
        )

    def plane_total(source, target, sems, stage):
        others = pl.ds(0, per_group - 1)
        return remote(
            source.at[stage, others],
            target.at[stage, others],
            sems.at[0],
            sems.at[stage + 1],
            plane_peer(1)[1],
        )

    def plane_sent(source, target, sems):
        others = pl.ds(0, per_group - 1)
        return remote(
            source.at[:, others], target.at[:, others], sems.at[0], sems.at[1], plane_peer(1)[1]
        )

    def each_column(act):
        for step in ORDER:
            act(step)

    def each_plane(act):
        def body(step, carry):
            act(step)
            return carry

        lax.fori_loop(1, per_group, body, 0)

    def load_all(pairs, sem):
        return [
            pltpu.make_async_copy(source, target, sem.at[index])
            for index, (source, target) in enumerate(pairs)
        ]

    barrier = pltpu.get_barrier_semaphore()

    def greet_column(step):
        pl.semaphore_signal(barrier, inc=1, device_id=(column_peer(step)[1],), device_id_type=MESH)

    def greet_plane(step):
        pl.semaphore_signal(barrier, inc=1, device_id=(plane_peer(step)[1],), device_id_type=MESH)

    smalls = load_all(
        (
            (expert_group_hbm, expert_group),
            (tokens_hbm, tokens),
            (expert_inner_hbm, expert_inner),
            (route_weights_hbm, route_weights),
            (norm_gain_hbm, norm_gain),
            (history_length_hbm, history_length),
            (inverse_hbm, inverse),
            (head_gain_hbm, head_gain),
            (moe_gain_hbm, moe_gain),
        ),
        small_sem,
    )
    weight_copies = load_all(
        (
            (query_hbm, query_w),
            (key_hbm, key_w),
            (value_hbm, value_w),
            (gate_hbm, gate_w),
            (out_hbm, out_w),
        ),
        weight_sem,
    )
    loads = load_all(
        (
            (expert_gate_hbm, expert_gate_w),
            (expert_up_hbm, expert_up_w),
            (expert_down_hbm, expert_down_w),
        ),
        load_sem,
    )

    def state_in(block):
        span = pl.ds(block * BLOCK, BLOCK)
        return pltpu.make_async_copy(state_hbm.at[span], state.at[span], in_sem.at[block])

    for copy in smalls + weight_copies[:1]:
        copy.start()
    each_column(greet_column)
    each_plane(greet_plane)
    for copy in weight_copies[1:3]:
        copy.start()

    square = (seq_count, seq_count)
    above = lax.broadcasted_iota(jnp.int32, square, 0)
    across = lax.broadcasted_iota(jnp.int32, square, 1)

    def column(row):
        return jnp.sum(jnp.where(above == across, row, 0.0), axis=1, keepdims=True)

    def earlier(columns, row):
        matched = sum((values == row).astype(jnp.float32) for values in columns)
        return jnp.sum(jnp.where(above < across, matched, 0.0), axis=0, keepdims=True)

    smalls[0].wait()
    group_row = expert_group[...].astype(jnp.float32)
    group_slot = group_row * group_rows + earlier([column(group_row)], group_row)
    slot_above = lax.broadcasted_iota(jnp.int32, (slots, seq_count), 0).astype(jnp.float32)
    placing = (slot_above == group_slot).astype(jnp.float32).astype(jnp.bfloat16)
    smalls[1].wait()
    zsend[...] = dot(placing, tokens[...]).astype(jnp.bfloat16).reshape(zsend.shape)
    with jax.named_scope("barrier"):
        pl.semaphore_wait(barrier, GROUPS - 1 + per_group - 1)
    outer = within == 0

    def send_tokens(stage, held):
        @pl.when(outer if held else jnp.logical_not(outer))
        def start():
            column_copy(zsend, zrecv, z_sems, stage).start()

    send_tokens(3, True)
    send_tokens(1, False)
    for block in range(2):
        state_in(block).start()
    for small in smalls[2:4]:
        small.wait()
    inner_rows = [expert_inner[choice : choice + 1, :].astype(jnp.float32) for choice in (0, 1)]
    expert_rows = [group_row * per_group + row for row in inner_rows]
    expert_columns = [column(row) for row in expert_rows]
    lanes = []
    for choice in (0, 1):
        slot = earlier(expert_columns, expert_rows[choice])
        lanes.append(column(inner_rows[choice] * capacity + slot + 1.0))
    for choice in (0, 1):
        weight = column(route_weights[choice : choice + 1, :])
        high = weight.astype(jnp.bfloat16).astype(jnp.float32)
        lanes += [high, weight - high]
    lane = lax.broadcasted_iota(jnp.int32, (seq_count, meta_send.shape[-1]), 1)
    token_meta = jnp.zeros(lane.shape, jnp.float32)
    for index, value in enumerate(lanes):
        token_meta = jnp.where(lane == index, value, token_meta)
    meta = dot(placing, token_meta.astype(jnp.bfloat16)).astype(jnp.bfloat16)
    meta_send[...] = meta.reshape(meta_send.shape)
    each_column(lambda step: column_copy(meta_send, meta_recv, meta_sems, step).start())
    meta_recv[0] = meta_send[group]
    zrecv[0] = zsend[group]

    def packed_places(shape, axis):
        index = lax.broadcasted_iota(jnp.int32, shape, axis)
        part = sum((index >= tiles * bound).astype(jnp.int32) for bound in range(1, parts))
        index = index - part * tiles
        place = (index & (BLOCK - 1)) * parts + part
        return (index >> 3) * capacity + (place >> 2), place & (QUARTERS - 1)

    packed_rows, packed_quarter = packed_places((1, parts * tiles), 1)
    row_names = packed_rows.astype(jnp.float32) + 1.0
    in_quarter = [(packed_quarter == part).astype(jnp.float32) for part in range(QUARTERS)]
    row_number = lax.broadcasted_iota(jnp.int32, (rows, parts * tiles), 0)
    same_row = (row_number == packed_rows).astype(jnp.float32)
    packing = jnp.concatenate([same_row * part for part in in_quarter], axis=0).astype(jnp.bfloat16)
    picks_of = {}
    weights_of = {}

    def stacked(block):
        share = block.shape[-1] // QUARTERS
        return jnp.concatenate(
            [block[:, part * share : (part + 1) * share] for part in range(QUARTERS)], axis=0
        )

    def unstacked(block):
        share = block.shape[0] // QUARTERS
        return jnp.concatenate(
            [block[part * share : (part + 1) * share] for part in range(QUARTERS)], axis=1
        )

    def take(picks, block):
        return lax.dot_general(
            picks, block, (((0,), (0,)), ((), ())), preferred_element_type=jnp.float32
        ).astype(jnp.bfloat16)

    def store_packed(sent, stage, block):
        share = block.shape[-1]
        for part in range(parts):
            sent[stage, :, :, part * share : (part + 1) * share] = block[
                part * tiles : (part + 1) * tiles
            ].reshape(per_group, BLOCK, share)

    def load_packed(landed, stage):
        block = landed[stage].reshape(tiles, landed.shape[-1])
        share = block.shape[-1] // parts
        return jnp.concatenate(
            [block[:, part * share : (part + 1) * share] for part in range(parts)], axis=0
        )

    def route(stage):
        if stage:
            column_landed(meta_send, meta_recv, meta_sems, stage).wait_recv()
        meta = meta_recv[stage].astype(jnp.float32)
        first = (row_names == meta[:, 0:1]).astype(jnp.float32)
        second = (row_names == meta[:, 1:2]).astype(jnp.float32)
        weights = first * (meta[:, 2:3] + meta[:, 3:4]) + second * (meta[:, 4:5] + meta[:, 5:6])
        both = first + second
        picks = jnp.concatenate([both * part for part in in_quarter], axis=0)
        weights = jnp.concatenate([weights * part for part in in_quarter], axis=0)
        high = weights.astype(jnp.bfloat16)
        picks_of[stage] = picks.astype(jnp.bfloat16)
        weights_of[stage] = (high, (weights - high.astype(jnp.float32)).astype(jnp.bfloat16))

    def spread(stage, picks, received, sent, landed, sems):
        block = stacked(received[stage].astype(jnp.float32)).astype(jnp.bfloat16)
        store_packed(sent, stage, take(picks, block))
        each_plane(lambda step: plane_copy(sent, landed, sems, stage, step).start())
        landed[stage, inner] = sent[stage, inner]

    def spread_tokens(stage):
        route(stage)
        if stage:
            column_landed(zsend, zrecv, z_sems, stage).wait_recv()
        spread(stage, picks_of[stage], zrecv, dsend, drecv, d_sems)

    def spread_nearer(first):
        stage = jnp.where(outer == first, 1, 2)
        near, far = (picks_of[1], picks_of[2]) if first else (picks_of[2], picks_of[1])
        picks = jnp.where(outer, near.astype(jnp.float32), far.astype(jnp.float32))
        column_landed(zsend, zrecv, z_sems, stage).wait_recv()
        spread(stage, picks.astype(jnp.bfloat16), zrecv, dsend, drecv, d_sems)

    def spread_heads(stage):
        if stage:
            column_landed(hsend, hrecv, h_sems, stage).wait_recv()
        spread(stage, picks_of[stage], hrecv, esend, erecv, e_sems)

    for small in smalls[4:]:
        small.wait()
    inputs = tokens[...].astype(jnp.float32)
    normed = rms(inputs, norm_gain[...]).astype(jnp.bfloat16)
    places = column(history_length[...].astype(jnp.float32))
    angles = places * inverse[...]
    cosine, sine = jnp.cos(angles), jnp.sin(angles)
    cosines = jnp.concatenate([cosine] * (2 * heads), axis=1)
    sines = jnp.concatenate([-sine, sine] * heads, axis=1)
    head_lane = lax.broadcasted_iota(jnp.int32, cosines.shape, 1)
    leading = lax.rem(head_lane, head_width) < half

    def rounded(weights):
        return dot(normed, weights[...]).astype(jnp.bfloat16).astype(jnp.float32)

    def rotated(values):
        partner = jnp.where(
            leading, jnp.roll(values, -half, axis=1), jnp.roll(values, half, axis=1)
        )
        return values * cosines + partner * sines

    def head_lanes(head):
        return slice(head * head_width, (head + 1) * head_width)

    with jax.named_scope("wait_q"):
        weight_copies[0].wait()
    queries = rotated(rounded(query_w))
    for head in range(heads):
        query_heads[head] = queries[:, head_lanes(head)]
    send_tokens(2, True)
    send_tokens(2, False)
    for block in range(2, blocks):
        if block == blocks - 2:
            weight_copies[3].start()
        state_in(block).start()
    with jax.named_scope("wait_k"):
        weight_copies[1].wait()
    keys = rotated(rounded(key_w)) * head_width ** (-0.5)
    with jax.named_scope("wait_v"):
        weight_copies[2].wait()
    values = rounded(value_w)
    products = keys * queries
    for head in range(heads):
        value_heads[head] = values[:, head_lanes(head)]
        overlap[head] = jnp.sum(products[:, head_lanes(head)], axis=1, keepdims=True)
    retain = [
        jnp.exp(jnp.full((1, head_width), -decay_rate[head], jnp.float32)) for head in range(heads)
    ]
    wide = (BLOCK, BLOCK * head_width)
    own = lax.broadcasted_iota(jnp.int32, wide, 0) == (
        lax.broadcasted_iota(jnp.int32, wide, 1) // head_width
    )

    def read(block, carry):
        state_in(block).wait()
        span = pl.ds(block * BLOCK, BLOCK)
        for head in range(heads):
            block_queries = query_heads[head, span, :]
            spread_queries = jnp.where(own, jnp.concatenate([block_queries] * BLOCK, axis=1), 0.0)
            high = spread_queries.astype(jnp.bfloat16).astype(jnp.float32)
            both = jnp.concatenate([high, spread_queries - high], axis=0).astype(jnp.bfloat16)
            old = state[span, head].reshape(BLOCK * head_width, head_width).astype(jnp.bfloat16)
            found = dot(both, old)
            reading[head, span, :] = (
                retain[head] * (found[:BLOCK] + found[BLOCK:])
                + overlap[head, span, :] * value_heads[head, span, :]
            )
        return carry

    def update(block, carry):
        span = pl.ds(block * BLOCK, BLOCK)
        for head in range(heads):
            lanes = slice(head * head_width, (head + 1) * head_width)
            block_values = value_heads[head, span, :]
            block_keys = key_columns[block, lanes, :]
            for index in range(BLOCK):
                sequence = block * BLOCK + index
                state[sequence, head] = (
                    retain[head] * state[sequence, head]
                    + block_keys[:, index : index + 1] * block_values[index : index + 1, :]
                )
        return carry

    def advance(first, last):
        with jax.named_scope(f"advance_{first}"):
            lax.fori_loop(first, last, update, 0)

    with jax.named_scope("spread_tokens_0"):
        spread_tokens(0)
    send_tokens(3, False)
    with jax.named_scope("read_a"):
        lax.fori_loop(0, blocks // 2, read, 0)
    send_tokens(1, True)
    with jax.named_scope("spread_near"):
        for stage in (1, 2):
            route(stage)
        spread_nearer(True)
    with jax.named_scope("read"):
        lax.fori_loop(blocks // 2, blocks, read, 0)
    for copy in weight_copies[4:] + loads:
        copy.start()
    with jax.named_scope("wait_g"):
        weight_copies[3].wait()
    gating = rounded(gate_w)
    read_heads = jnp.concatenate(
        [
            rms(
                reading[head],
                head_gain[:, head_lanes(head)],
            )
            for head in range(heads)
        ],
        axis=1,
    )
    mixed_heads = (read_heads * jax.nn.silu(gating)).astype(jnp.bfloat16)
    hsend[...] = dot(placing, mixed_heads).astype(jnp.bfloat16).reshape(hsend.shape)
    each_column(lambda step: column_copy(hsend, hrecv, h_sems, step).start())
    hrecv[0] = hsend[group]
    half_width = width // HALVES

    def run_expert(*stages):
        token_rows, head_rows = [], []
        for stage in stages:
            plane_total(dsend, drecv, d_sems, stage).wait_recv()
            token_rows.append(unstacked(dot(packing, load_packed(drecv, stage))))
        for stage in stages:
            plane_total(esend, erecv, e_sems, stage).wait_recv()
            head_rows.append(unstacked(dot(packing, load_packed(erecv, stage))))
        head_rows = jnp.concatenate(head_rows, axis=0).astype(jnp.bfloat16)
        token_rows = jnp.concatenate(token_rows, axis=0)
        block = (token_rows + dot(head_rows, out_w[...])).astype(jnp.bfloat16)
        block = rms(block.astype(jnp.float32), moe_gain[...]).astype(jnp.bfloat16)
        hidden = jax.nn.silu(dot(block, expert_gate_w[...])) * dot(block, expert_up_w[...])
        hidden = hidden.astype(jnp.bfloat16)
        for half in range(HALVES):
            lanes = slice(half * half_width, (half + 1) * half_width)
            block = dot(hidden, expert_down_w[:, lanes])
            for place, stage in enumerate(stages):
                share = block[place * rows : (place + 1) * rows].astype(jnp.bfloat16)
                store_packed(osend, stage * HALVES + half, take(packing, stacked(share)))
            if stages[0]:
                for stage in stages:
                    send_back(stage, half)

    def send_back(stage, half):
        index = stage * HALVES + half
        each_plane(lambda step: plane_copy(osend, orecv, o_sems, index, step).start())
        orecv[index, inner] = osend[index, inner]

    def combine(stage, half):
        index = stage * HALVES + half
        plane_total(osend, orecv, o_sems, index).wait_recv()
        block = load_packed(orecv, index)
        high, low = weights_of[stage]
        block = unstacked(dot(high, block) + dot(low, block)).astype(jnp.bfloat16)
        if stage:
            csend[stage, half] = block
            send_home(stage, half).start()
        else:
            crecv[group, half] = block

    def combine_all(stage):
        for half in range(HALVES):
            with jax.named_scope(f"combine_{stage}_{half}"):
                combine(stage, half)

    with jax.named_scope("spread_heads_0"):
        spread_heads(0)
    with jax.named_scope("spread_far"):
        spread_nearer(False)
    for block in range(blocks):
        key_columns[block] = keys[block * BLOCK : (block + 1) * BLOCK].T
    advance(0, blocks // 2)
    for stage in (2, 1):
        with jax.named_scope(f"spread_heads_{stage}"):
            spread_heads(stage)
    with jax.named_scope("spread_tokens_3"):
        spread_tokens(3)
    with jax.named_scope("wait_oe"):
        for copy in weight_copies[4:] + loads:
            copy.wait()

    with jax.named_scope("run_expert_0"):
        run_expert(0)
    with jax.named_scope("spread_heads_3"):
        spread_heads(3)
    with jax.named_scope("run_expert_2"):
        run_expert(2)
    with jax.named_scope("run_expert_31"):
        run_expert(1, 3)
    combine_all(2)
    for half in range(HALVES):
        send_back(0, half)
    with jax.named_scope("mixed"):
        mixed = (inputs + dot(mixed_heads, out_w[...])).astype(jnp.bfloat16)
    advance(blocks // 2, 4 * blocks // 6)
    for half in range(HALVES):
        for stage in (1, 3):
            with jax.named_scope(f"combine_{stage}_{half}"):
                combine(stage, half)
        advance((4 + half) * blocks // 6, (5 + half) * blocks // 6)
    combine_all(0)
    slot_across = lax.broadcasted_iota(jnp.int32, (seq_count, slots), 1).astype(jnp.float32)
    collecting = (slot_across == column(group_slot)).astype(jnp.float32).astype(jnp.bfloat16)
    for half in range(HALVES):
        lanes = slice(half * half_width, (half + 1) * half_width)
        with jax.named_scope(f"wait_home_{half}"):
            each_column(lambda step: home_landed(step, half).wait_recv())
        block = dot(collecting, crecv[:, half].reshape(slots, half_width))
        out[:, lanes] = (mixed[:, lanes].astype(jnp.float32) + block).astype(jnp.bfloat16)
    column_sent(meta_send, meta_recv, meta_sems).wait_send()
    column_sent(zsend, zrecv, z_sems).wait_send()
    column_sent(hsend, hrecv, h_sems).wait_send()
    column_sent(csend, crecv, c_sems).wait_send()
    plane_sent(dsend, drecv, d_sems).wait_send()
    plane_sent(esend, erecv, e_sems).wait_send()
    plane_sent(osend, orecv, o_sems).wait_send()


def finish_kernel(output, state, out, state_out, sem):
    blocks = sem.shape[0] - 1
    share = state.shape[0] // blocks
    copies = [pltpu.make_async_copy(output, out, sem.at[blocks])]
    for block in range(blocks):
        span = pl.ds(block * share, share)
        copies.append(pltpu.make_async_copy(state.at[span], state_out.at[span], sem.at[block]))
    for copy in copies:
        copy.start()
    for copy in copies:
        copy.wait()


def finish(output, new_state):
    vmem = pl.BlockSpec(memory_space=pltpu.VMEM)
    hbm = pl.BlockSpec(memory_space=pl.ANY)
    return pl.pallas_call(
        finish_kernel,
        name="finish",
        out_shape=(
            jax.ShapeDtypeStruct(output.shape, output.dtype),
            jax.ShapeDtypeStruct(new_state.shape, new_state.dtype),
        ),
        in_specs=[vmem, vmem],
        out_specs=(hbm, hbm),
        scratch_shapes=[pltpu.SemaphoreType.DMA((2 * new_state.shape[0] // BLOCK + 1,))],
        compiler_params=pltpu.CompilerParams(vmem_limit_bytes=4 * 1024 * 1024),
    )(output, new_state)


def local(
    tokens,
    history_length,
    norm_gain,
    w_query,
    w_key,
    w_value,
    w_gate,
    decay_rate,
    state,
    head_gain,
    w_out,
    moe_gain,
    route_weights,
    expert_group,
    expert_inner,
    expert_gate,
    expert_up,
    expert_down,
):
    experts = lax.axis_size("ep")
    per_group = experts // GROUPS
    heads = decay_rate.shape[0]
    seq_count, model_width = tokens.shape
    head_width = state.shape[-1]
    mixed_width = heads * head_width
    half = head_width // 2
    blocks = seq_count // BLOCK
    inverse = (10000.0 ** (-np.arange(half) / half)).astype(np.float32)
    capacity = max(2, 4 * seq_count // experts)
    group_rows = -(-min(seq_count, per_group * capacity // TOP_K) // 8) * 8
    capacity += capacity % 2
    packed = capacity * QUARTERS // BLOCK
    half_lanes = model_width // HALVES * packed // QUARTERS
    vmem = pl.BlockSpec(memory_space=pltpu.VMEM)
    smem = pl.BlockSpec(memory_space=pltpu.SMEM)
    hbm = pl.BlockSpec(memory_space=pl.ANY)
    dma = pltpu.SemaphoreType.DMA
    bf16, f32 = jnp.bfloat16, jnp.float32

    def column_buffer(lanes):
        return [pltpu.VMEM((GROUPS, group_rows, lanes), bf16)] * 2

    def plane_buffer(lanes):
        return [pltpu.VMEM((STAGES, per_group, BLOCK, lanes * packed // QUARTERS), bf16)] * 2

    weights = (w_query, w_key, w_value, w_gate, w_out, expert_gate[0], expert_up[0], expert_down[0])
    state_bytes = state.size // head_width * max(head_width, 128) * 4

    smalls = (
        tokens,
        history_length.reshape(1, -1),
        inverse.reshape(1, -1),
        norm_gain.reshape(1, -1),
        head_gain.reshape(1, -1),
        moe_gain.reshape(1, -1),
        expert_group.reshape(1, -1),
        expert_inner.T,
        route_weights.T,
    )

    def kernel(*refs):
        layer_kernel(per_group, capacity, *refs)

    output, new_state = pl.pallas_call(
        kernel,
        name="layer",
        out_shape=(
            pltpu.VMEM((seq_count, model_width), bf16),
            pltpu.VMEM(state.shape, f32),
        ),
        in_specs=[smem] + [hbm] * 18,
        out_specs=(vmem, vmem),
        scratch_shapes=[pltpu.VMEM(weight.shape, bf16) for weight in weights]
        + [pltpu.VMEM(small.shape, small.dtype) for small in smalls]
        + [
            pltpu.VMEM((blocks, mixed_width, BLOCK), f32),
            pltpu.VMEM((heads, seq_count, head_width), f32),
            pltpu.VMEM((heads, seq_count, head_width), f32),
            pltpu.VMEM((heads, seq_count, head_width), f32),
            pltpu.VMEM((heads, seq_count, 1), f32),
        ]
        + column_buffer(128)
        + column_buffer(model_width)
        + column_buffer(mixed_width)
        + plane_buffer(model_width)
        + plane_buffer(mixed_width)
        + [pltpu.VMEM((STAGES * HALVES, per_group, BLOCK, half_lanes), bf16)] * 2
        + [pltpu.VMEM((GROUPS, HALVES, group_rows, model_width // HALVES), bf16)] * 2
        + [
            dma((9,)),
            dma((5,)),
            dma((blocks,)),
            dma((3,)),
            dma((GROUPS,)),
            dma((GROUPS,)),
            dma((GROUPS,)),
            dma((STAGES + 1,)),
            dma((STAGES + 1,)),
            dma((STAGES * HALVES + 1,)),
            dma((GROUPS * HALVES,)),
        ],
        compiler_params=pltpu.CompilerParams(
            collective_id=0,
            has_side_effects=True,
            vmem_limit_bytes=63 * 1024 * 1024 - state_bytes,
        ),
    )(
        decay_rate,
        *smalls,
        w_query,
        w_key,
        w_value,
        w_gate,
        w_out,
        state,
        expert_gate[0],
        expert_up[0],
        expert_down[0],
    )
    return finish(output, new_state)


def solution(mesh):
    return jax.shard_map(
        local,
        mesh=mesh,
        in_specs=(
            P("ep", None),
            P("ep"),
            P(),
            P(),
            P(),
            P(),
            P(),
            P(),
            P("ep", None, None, None),
            P(),
            P(),
            P(),
            P("ep", None),
            P("ep"),
            P("ep", None),
            P("ep", None, None),
            P("ep", None, None),
            P("ep", None, None),
        ),
        out_specs=(P("ep", None), P("ep", None, None, None)),
        check_vma=False,
    )
```
